32 devices in a mesh: sp: 8 (over z, x), tp: 4 (over y, core).
Axes of the slice: x: 2, y: 2, z: 4, core: 2. Of those that a mesh axis runs over, the one named last changes fastest.
Arguments:
- tokens: bfloat16 [1024, 2048], P(('sp', 'tp')), may hold values from -6 to 6
- pre_gain: bfloat16 [2048], replicated, may hold values from 0.099609375 to 1.8984375
- w_query: bfloat16 [2048, 1024], P('sp', 'tp'), may hold values from -0.125 to 0.125
- w_key: bfloat16 [2048, 1024], P('sp', 'tp'), may hold values from -0.125 to 0.125
- w_value: bfloat16 [2048, 2048], P('sp', 'tp'), may hold values from -0.125 to 0.125
- w_igate: bfloat16 [2048, 8], replicated, may hold values from -1 to 1
- w_fgate: bfloat16 [2048, 8], replicated, may hold values from -0.125 to 0.125
- forget_bias: float32 [8], replicated, may hold values from 4 to 16
- gate_drift: float32 [1024, 8], P('sp'), may hold values from -2 to 2, as said below
- head_gain: bfloat16 [2048], replicated, may hold values from 0.099609375 to 1.8984375
- w_out: bfloat16 [2048, 2048], P('sp', 'tp'), may hold values from -0.125 to 0.125
Outputs:
- layer_out: bfloat16 [1024, 2048], P(('sp', 'tp'))
The draws below stay inside these ranges and needn't reach their ends.
Inputs may be any that keep to these rules, and one draw needn't show every extreme that they name: `gate_drift`: constant over aligned spans of 128 positions.
All inputs are finite; a program needn't handle non-finite values.
Results may differ from the reference program's by a relative error of at most 0.02.
Values may be sent and summed in bfloat16 or wider, within the bound.
A program may use at most 64 MiB of HBM per device.

```python
import math
import jax
import jax.numpy as jnp
from jax import lax

D = 2048
HEADS = 8
DK = 128
DV = 256
BLOCK = 64
TOKENS = 1024
HEADS_DEV = 2
N_TP = 4


def gate_columns(key):
    return jax.random.normal(jax.random.fold_in(key, 7), (D, HEADS), jnp.float32)


def draw_w_igate(key, part):
    base_cols = gate_columns(key)
    spread_scale = 1.0
    return jnp.clip(base_cols * (spread_scale / math.sqrt(D)), -1.0, 1.0).astype(jnp.bfloat16)


def draw_tokens(key, part):
    rough_rows = jax.random.normal(jax.random.fold_in(key, 1), (TOKENS, D), jnp.float32)
    return jnp.clip(rough_rows, -6.0, 6.0).astype(jnp.bfloat16)


def draw_forget_bias(key, part):
    head_order = jax.random.permutation(jax.random.fold_in(key, 4), HEADS)
    slow_count = HEADS // 2
    slow_heads = head_order < slow_count
    jitter = jax.random.uniform(jax.random.fold_in(key, 5), (HEADS,), jnp.float32, -0.3, 0.3)
    return jnp.where(slow_heads, math.log(TOKENS) + 0.8, math.log(100.0)) + jitter


def draw_gate_drift(key, part):
    span_count = TOKENS // (2 * BLOCK)
    span_level = jax.random.uniform(jax.random.fold_in(key, 6), (span_count, HEADS), jnp.float32, -1.5, 1.5)
    return jnp.repeat(span_level, 2 * BLOCK, axis=0)


def block_scale(key, shape, shards, low, high):
    def one(position, blocks):
        heights = jax.random.uniform(jax.random.fold_in(jax.random.fold_in(key, 6), position), (blocks,), jnp.float32, low / len(shards), high / len(shards))
        return jnp.repeat(jnp.exp(heights), shape[position] // blocks).reshape((-1,) + (1,) * (len(shape) - position - 1))

    level = one(*shards[0])
    for cut in shards[1:]:
        level = level * one(*cut)
    return level


def noise(stream_key, extent, spread, most, cuts=(), dtype=jnp.bfloat16):
    factor_of = block_scale(stream_key, extent, cuts, -0.22, 0.18) if cuts else 1.0
    entries = jax.random.normal(stream_key, extent, jnp.float32) * spread * factor_of
    return jnp.minimum(jnp.maximum(entries, -most), most).astype(dtype)


def setup_inputs(seed: int = 0) -> dict:
    streams_of = jax.random.split(jax.random.key(seed), 12)
    tokens = draw_tokens(jax.random.fold_in(streams_of[11], 71), 0)
    pre_gain = jnp.clip(1.0 + 0.18 * jax.random.normal(streams_of[1], (D,), jnp.float32), 0.099609375, 1.8984375).astype(jnp.bfloat16)
    w_query = noise(streams_of[2], (D, HEADS * DK), D ** -0.5, 0.125, ((0, 8), (1, 4)))
    w_key = noise(streams_of[3], (D, HEADS * DK), D ** -0.5, 0.125, ((0, 8), (1, 4)))
    w_value = noise(streams_of[4], (D, HEADS * DV), D ** -0.5, 0.125, ((0, 8), (1, 4)))
    w_igate = draw_w_igate(jax.random.fold_in(streams_of[11], 71), 0)
    w_fgate = noise(streams_of[6], (D, HEADS), D ** -0.5, 0.125)
    forget_bias = draw_forget_bias(jax.random.fold_in(streams_of[11], 71), 0)
    gate_drift = draw_gate_drift(jax.random.fold_in(streams_of[11], 71), 0)
    head_gain = jnp.clip(1.0 + 0.18 * jax.random.normal(streams_of[9], (HEADS * DV,), jnp.float32), 0.099609375, 1.8984375).astype(jnp.bfloat16)
    w_out = noise(streams_of[10], (D, HEADS * DV), (HEADS * DV) ** -0.5, 0.125, ((0, 8), (1, 4)))
    return dict(tokens=tokens, pre_gain=pre_gain, w_query=w_query, w_key=w_key, w_value=w_value, w_igate=w_igate, w_fgate=w_fgate, forget_bias=forget_bias, gate_drift=gate_drift, head_gain=head_gain, w_out=w_out)


norm_floor = 0.1
lowest_log = -1e+30
highest = lax.Precision.HIGHEST

def advance(memory, summary):
    old_mat, old_vec, old_top = memory
    span_log, span_top, span_mat, span_vec = summary
    new_top = jnp.maximum(span_log + old_top, span_top)
    kept_part = jnp.exp(span_log + old_top - new_top)
    fresh_part = jnp.exp(span_top - new_top)
    return (kept_part[:, None, None] * old_mat + fresh_part[:, None, None] * span_mat, kept_part[:, None] * old_vec + fresh_part[:, None] * span_vec, new_top)

def blend_parts(first_part, second_part):
    numer_first, denom_first, peak_first = first_part
    numer_second, denom_second, peak_second = second_part
    new_top = jnp.maximum(peak_first, peak_second)
    weight_first = jnp.exp(peak_first - new_top)
    weight_second = jnp.exp(peak_second - new_top)
    return (weight_first[..., None] * numer_first + weight_second[..., None] * numer_second, weight_first * denom_first + weight_second * denom_second, new_top)

def reference(tokens, pre_gain, w_query, w_key, w_value, w_igate, w_fgate, forget_bias, gate_drift, head_gain, w_out):
    token_wide = tokens.astype(jnp.float32)
    scaled = token_wide * lax.rsqrt(lax.optimization_barrier(jnp.mean(token_wide * token_wide, axis=1, keepdims=True)) + norm_floor)
    normed = (scaled * pre_gain.astype(jnp.float32)).astype(jnp.bfloat16)
    queries = jnp.dot(normed, w_query, preferred_element_type=jnp.float32).astype(jnp.bfloat16)
    keys_all = (jnp.dot(normed, w_key, preferred_element_type=jnp.float32) * DK ** (-0.5)).astype(jnp.bfloat16)
    values_all = jnp.dot(normed, w_value, preferred_element_type=jnp.float32).astype(jnp.bfloat16)
    log_input = jnp.dot(normed, w_igate, preferred_element_type=jnp.float32)
    forget_pre = jnp.dot(normed, w_fgate, preferred_element_type=jnp.float32) + forget_bias
    log_forget = jax.nn.log_sigmoid(forget_pre + gate_drift)
    blocks = TOKENS // BLOCK
    head_gains = head_gain.astype(jnp.float32).reshape(HEADS, DV)
    causal = jnp.arange(BLOCK)[:, None] >= jnp.arange(BLOCK)[None, :]

    def block_step(carry_state, inputs):
        memory_mat, memory_vec, memory_top = carry_state
        query_blk, key_blk, value_blk, input_row, forget_row = inputs
        query_wide = query_blk.astype(jnp.float32)
        key_wide = key_blk.astype(jnp.float32)
        value_wide = value_blk.astype(jnp.float32)
        input_gate = input_row.T
        forget_gate = forget_row.T
        within = jnp.cumsum(forget_gate, axis=1)
        log_pair = jnp.where(causal, within[:, :, None] - within[:, None, :] + input_gate[:, None, :], -jnp.inf)
        peak_intra = lax.optimization_barrier(jnp.max(log_pair, axis=2))
        scores = jnp.einsum('shd,rhd->hsr', query_wide, key_wide, precision=highest)
        weights = scores * jnp.exp(log_pair - peak_intra[:, :, None])
        weights_low = lax.optimization_barrier(weights.astype(jnp.bfloat16))
        numer_intra = jnp.einsum('hsr,rhv->hsv', weights_low.astype(jnp.float32), value_wide, precision=highest)
        denom_intra = lax.optimization_barrier(jnp.sum(weights, axis=2))
        carried_log = within + memory_top[:, None]
        numer_carry = jnp.einsum('hvd,shd->hsv', memory_mat, query_wide, precision=highest)
        denom_carry = jnp.einsum('hd,shd->hs', memory_vec, query_wide, precision=highest)
        numerator, denominator, peak_log = blend_parts((numer_carry, denom_carry, carried_log), (numer_intra, denom_intra, peak_intra))
        hidden = numerator / jnp.maximum(jnp.abs(denominator), jnp.exp(-peak_log))[:, :, None]
        hidden = hidden.transpose(1, 0, 2)
        normed_heads = hidden * lax.rsqrt(lax.optimization_barrier(jnp.mean(hidden * hidden, axis=2, keepdims=True)) + norm_floor) * head_gains
        span_log = within[:, -1]
        log_write = span_log[:, None] - within + input_gate
        span_top = lax.optimization_barrier(jnp.max(log_write, axis=1))
        write_scale = jnp.exp(log_write - span_top[:, None])
        key_scaled = key_wide * write_scale.T[:, :, None]
        span_mat = jnp.einsum('rhv,rhd->hvd', value_wide, key_scaled, precision=highest)
        span_vec = lax.optimization_barrier(jnp.sum(key_scaled, axis=0))
        new_state = advance(carry_state, (span_log, span_top, span_mat, span_vec))
        return (new_state, normed_heads.astype(jnp.bfloat16).reshape(BLOCK, HEADS * DV))
    init_state = (jnp.zeros((HEADS, DV, DK), jnp.float32), jnp.zeros((HEADS, DK), jnp.float32), jnp.full((HEADS,), lowest_log, jnp.float32))
    scanned = (queries.reshape(blocks, BLOCK, HEADS, DK), keys_all.reshape(blocks, BLOCK, HEADS, DK), values_all.reshape(blocks, BLOCK, HEADS, DV), log_input.reshape(blocks, BLOCK, HEADS), log_forget.reshape(blocks, BLOCK, HEADS))
    outputs = lax.scan(block_step, init_state, scanned)[1]
    normed_all = outputs.reshape(TOKENS, HEADS * DV)
    group_width = HEADS_DEV * DV
    total_sum = jnp.zeros((TOKENS, D), jnp.float32)
    for group_index in range(N_TP):
        columns = slice(group_index * group_width, (group_index + 1) * group_width)
        partial_value = lax.dot_general(normed_all[:, columns], w_out[:, columns], (((1,), (1,)), ((), ())), preferred_element_type=jnp.float32)
        partial_value = lax.optimization_barrier(partial_value.astype(jnp.bfloat16))
        total_sum = total_sum + partial_value.astype(jnp.float32)
    return total_sum.astype(jnp.bfloat16)
```

```python
import functools

import jax
import jax.numpy as jnp
from jax import lax
from jax.experimental import pallas as pl
from jax.experimental.pallas import tpu as pltpu
from jax.sharding import PartitionSpec as P

BLOCK = 64


norm_floor = 0.1
lowest_log = -1e30
highest = lax.Precision.HIGHEST


def prefix(value, axis, combine, identity):
    peers, position = (lax.axis_size(axis), lax.axis_index(axis))
    everything = jax.tree.map(
        lambda part, kind: lax.all_gather(part.astype(kind), axis),
        value,
        jax.tree.map(lambda a: jnp.bfloat16 if a.dtype == jnp.float32 else a.dtype, value),
    )
    start = jax.tree.map(
        lambda part, zero: jnp.broadcast_to(jnp.asarray(zero, part.dtype), part.shape),
        value,
        identity,
    )

    def step(k, before):
        reached = k < position
        new = combine(
            before, jax.tree.map(lambda part, own: part[k].astype(own.dtype), everything, value)
        )
        return jax.tree.map(lambda a, b: jnp.where(reached, a, b), new, before)

    return lax.fori_loop(0, peers, step, start)


def advance(memory, summary):
    old_mat, old_vec, old_top = memory
    span_log, span_top, span_mat, span_vec = summary
    new_top = jnp.maximum(span_log + old_top, span_top)
    kept_part = jnp.exp(span_log + old_top - new_top)
    fresh_part = jnp.exp(span_top - new_top)
    return (
        kept_part[:, None, None] * old_mat + fresh_part[:, None, None] * span_mat,
        kept_part[:, None] * old_vec + fresh_part[:, None] * span_vec,
        new_top,
    )


def prefix_states(initial, summary):

    def stepper(memory, one_block):
        return (advance(memory, one_block), memory)

    return lax.scan(stepper, initial, summary)


def join_devices(earlier, later_part):
    early_log, early_mat, early_vec, early_top = earlier
    late_log, late_mat, late_vec, late_top = later_part
    new_top = jnp.maximum(late_log + early_top, late_top)
    kept_part = jnp.exp(late_log + early_top - new_top)
    fresh_part = jnp.exp(late_top - new_top)
    return (
        early_log + late_log,
        kept_part[:, None, None] * early_mat + fresh_part[:, None, None] * late_mat,
        kept_part[:, None] * early_vec + fresh_part[:, None] * late_vec,
        new_top,
    )


def blend_parts(first_part, second_part):
    numer_first, denom_first, peak_first = first_part
    numer_second, denom_second, peak_second = second_part
    new_top = jnp.maximum(peak_first, peak_second)
    weight_first = jnp.exp(peak_first - new_top)
    weight_second = jnp.exp(peak_second - new_top)
    return (
        weight_first[..., None] * numer_first + weight_second[..., None] * numer_second,
        weight_first * denom_first + weight_second * denom_second,
        new_top,
    )


def on_device(
    tokens,
    pre_gain,
    w_query,
    w_key,
    w_value,
    w_igate,
    w_fgate,
    forget_bias,
    gate_drift,
    head_gain,
    w_out,
):
    tp_size = lax.axis_size("tp")
    head_count = w_igate.shape[1]
    local_heads = head_count // tp_size
    first_head = lax.axis_index("tp") * local_heads
    key_width = w_query.shape[1] // local_heads
    value_width = w_value.shape[1] // local_heads
    token_wide = tokens.astype(jnp.float32)
    scaled = token_wide * lax.rsqrt(
        jnp.mean(token_wide * token_wide, axis=1, keepdims=True) + norm_floor
    )
    normed = (scaled * pre_gain.astype(jnp.float32)).astype(jnp.bfloat16)
    gate_cols = jnp.concatenate(
        [
            lax.dynamic_slice_in_dim(w_igate, first_head, local_heads, 1),
            lax.dynamic_slice_in_dim(w_fgate, first_head, local_heads, 1),
        ],
        axis=1,
    )
    key_scale = key_width ** (-0.5)
    wq_full, wk_full, wv_full = (
        lax.all_gather(w_query, "sp", axis=0, tiled=True),
        lax.all_gather(w_key, "sp", axis=0, tiled=True),
        lax.all_gather(w_value, "sp", axis=0, tiled=True),
    )
    row_piece = lax.all_gather(normed, "tp", axis=0, tiled=True)
    queries_part = jnp.dot(row_piece, wq_full, preferred_element_type=jnp.float32).astype(
        jnp.bfloat16
    )
    keys_part = (
        jnp.dot(row_piece, wk_full, preferred_element_type=jnp.float32) * key_scale
    ).astype(jnp.bfloat16)
    values_part = jnp.dot(row_piece, wv_full, preferred_element_type=jnp.float32).astype(
        jnp.bfloat16
    )
    gate_part = jnp.dot(row_piece, gate_cols, preferred_element_type=jnp.float32)
    group_len = queries_part.shape[0]
    blocks = group_len // BLOCK
    log_input = gate_part[:, :local_heads]
    forget_pre = gate_part[:, local_heads:] + lax.dynamic_slice_in_dim(
        forget_bias, first_head, local_heads, 0
    )
    log_forget = jax.nn.log_sigmoid(
        forget_pre + lax.dynamic_slice_in_dim(gate_drift, first_head, local_heads, 1)
    )
    query_blk = queries_part.reshape(blocks, BLOCK, local_heads, key_width)
    key_blk = keys_part.reshape(blocks, BLOCK, local_heads, key_width)
    value_blk = values_part.reshape(blocks, BLOCK, local_heads, value_width)
    input_blk = log_input.reshape(blocks, BLOCK, local_heads).transpose(0, 2, 1)
    forget_blk = log_forget.reshape(blocks, BLOCK, local_heads).transpose(0, 2, 1)
    within = jnp.cumsum(forget_blk, axis=2)
    causal = jnp.arange(BLOCK)[:, None] >= jnp.arange(BLOCK)[None, :]
    log_pair = jnp.where(
        causal, within[..., :, None] - within[..., None, :] + input_blk[..., None, :], -jnp.inf
    )
    peak_intra = jnp.max(log_pair, axis=3)
    scores = jnp.einsum("nshd,nrhd->nhsr", query_blk, key_blk, preferred_element_type=jnp.float32)
    weights = scores * jnp.exp(log_pair - peak_intra[..., None])
    numer_intra = jnp.einsum(
        "nhsr,nrhv->nhsv",
        weights.astype(jnp.bfloat16),
        value_blk,
        preferred_element_type=jnp.float32,
    )
    denom_intra = jnp.sum(weights, axis=3)
    span_log = within[..., -1]
    log_write = span_log[..., None] - within + input_blk
    span_top = jnp.max(log_write, axis=2)
    write_scale = jnp.exp(log_write - span_top[..., None])
    key_scaled = key_blk.astype(jnp.float32) * write_scale.transpose(0, 2, 1)[..., None]
    value_wide = value_blk.astype(jnp.float32)
    span_mat = jnp.einsum("nrhv,nrhd->nhvd", value_wide, key_scaled, precision=highest)
    span_vec = jnp.sum(key_scaled, axis=1)
    summary = (span_log, span_top, span_mat, span_vec)
    empty_state = (
        jnp.zeros((local_heads, value_width, key_width), jnp.float32),
        jnp.zeros((local_heads, key_width), jnp.float32),
        jnp.full((local_heads,), lowest_log, jnp.float32),
    )
    local_end, local_starts = prefix_states(empty_state, summary)
    device_summary = (jnp.sum(span_log, axis=0),) + local_end
    identity_all = (jnp.zeros((local_heads,), jnp.float32),) + empty_state
    incoming = prefix(device_summary, "sp", join_devices, identity_all)
    query_wide = query_blk.astype(jnp.float32)
    intra_part = (numer_intra, denom_intra, peak_intra)
    start_mat, start_vec, start_top = local_starts
    local_part = (
        jnp.einsum("nhvd,nshd->nhsv", start_mat, query_wide, precision=highest),
        jnp.einsum("nhd,nshd->nhs", start_vec, query_wide, precision=highest),
        within + start_top[..., None],
    )
    numerator, denominator, peak_log = blend_parts(local_part, intra_part)
    entry_log, entry_mat, entry_vec, entry_top = incoming
    before_log = jnp.concatenate(
        [jnp.zeros((1, local_heads), jnp.float32), jnp.cumsum(span_log, axis=0)[:-1]], axis=0
    )
    from_left = (
        jnp.einsum("hvd,nshd->nhsv", entry_mat, query_wide, precision=highest),
        jnp.einsum("hd,nshd->nhs", entry_vec, query_wide, precision=highest),
        within + (before_log + entry_top[None, :])[..., None],
    )
    numerator, denominator, peak_log = blend_parts((numerator, denominator, peak_log), from_left)
    hidden = numerator / jnp.maximum(jnp.abs(denominator), jnp.exp(-peak_log))[..., None]
    hidden = hidden.transpose(0, 2, 1, 3).reshape(group_len, local_heads, value_width)
    head_gains = lax.dynamic_slice_in_dim(
        head_gain, first_head * value_width, local_heads * value_width, 0
    )
    head_gains = head_gains.astype(jnp.float32).reshape(local_heads, value_width)
    normed_heads = (
        hidden
        * lax.rsqrt(jnp.mean(hidden * hidden, axis=2, keepdims=True) + norm_floor)
        * head_gains
    )
    normed_heads = normed_heads.astype(jnp.bfloat16).reshape(group_len, local_heads * value_width)
    out_slab = lax.all_gather(w_out, "sp", axis=0, tiled=True)
    return lax.psum_scatter(
        lax.dot_general(
            normed_heads, out_slab, (((1,), (1,)), ((), ())), preferred_element_type=jnp.float32
        ).astype(jnp.bfloat16),
        "tp",
        scatter_dimension=0,
        tiled=True,
    )


ring_limit = 16
MESH = pl.DeviceIdType.MESH
f32 = jnp.float32
bf16 = jnp.bfloat16


def dot_nt(a, b):
    return lax.dot_general(a, b, (((1,), (1,)), ((), ())), preferred_element_type=f32)


def ring_kernel(
    n,
    tp,
    lh,
    tokens,
    pre_gain,
    w_query,
    w_key,
    w_value,
    w_igate,
    w_fgate,
    forget_base,
    head_gain,
    w_out,
    out,
    tok_all,
    normed,
    key_in,
    value_in,
    query_in,
    out_in,
    state_own,
    state_in,
    aux_own,
    aux_in,
    acc,
    heads,
    shares,
    shares_in,
    tok_send,
    tok_recv,
    ring_send,
    ring_recv,
    aux_send,
    aux_recv,
    share_send,
    share_recv,
):
    s = lax.axis_index("sp")
    t = lax.axis_index("tp")
    half_ring = n // 2
    steps = n - 1
    odd = s % 2
    pos = odd * (n - 1) + (1 - 2 * odd) * (s // 2)

    def owner_at(p):
        p = lax.rem(p + 2 * n, n)
        far = p // half_ring
        return far * (2 * (n - 1 - p) + 1) + (1 - far) * 2 * p

    right = owner_at(pos + 1)
    left = owner_at(pos - 1)
    targets = (right, left)
    rows = tokens.shape[0]
    length = rows * tp
    dk = w_query.shape[1] // lh
    dv = w_value.shape[1] // lh
    depth = w_query.shape[0]
    half = depth // 2

    barrier = pltpu.get_barrier_semaphore()
    for peer in targets:
        pl.semaphore_signal(barrier, inc=1, device_id={"sp": peer}, device_id_type=MESH)
    for i in range(1, tp):
        pl.semaphore_signal(
            barrier, inc=1, device_id={"tp": lax.rem(t + i, tp)}, device_id_type=MESH
        )
    pl.semaphore_wait(barrier, 2 + tp - 1)

    copies = []

    def ring_copy(piece, own, landing, d, k):
        size = own.shape[0] // 2
        source = own.at[pl.ds(d * size, size)] if k == 0 else landing.at[d, k - 1]
        copy = pltpu.make_async_remote_copy(
            src_ref=source,
            dst_ref=landing.at[d, k],
            send_sem=ring_send.at[piece, d, k],
            recv_sem=ring_recv.at[piece, d, k],
            device_id={"sp": targets[d]},
            device_id_type=MESH,
        )
        copy.start()
        copies.append(copy)
        return copy

    def aux_copy(k):
        copy = pltpu.make_async_remote_copy(
            src_ref=aux_own if k == 0 else aux_in.at[k - 1],
            dst_ref=aux_in.at[k],
            send_sem=aux_send.at[k],
            recv_sem=aux_recv.at[k],
            device_id={"sp": right},
            device_id_type=MESH,
        )
        copy.start()
        copies.append(copy)
        return copy

    my_rows = pl.ds(pl.multiple_of(t * rows, rows), rows)
    token_copies = []
    for i in range(1, tp):
        copy = pltpu.make_async_remote_copy(
            src_ref=tokens,
            dst_ref=tok_all.at[my_rows],
            send_sem=tok_send.at[i - 1],
            recv_sem=tok_recv.at[i - 1],
            device_id={"tp": lax.rem(t + i, tp)},
            device_id_type=MESH,
        )
        copy.start()
        copies.append(copy)
        token_copies.append(copy)
    pieces = ((0, w_key, key_in), (1, w_value, value_in), (2, w_query, query_in))
    live = {}
    for piece, own, landing in pieces:
        for d in range(2):
            live[piece, d] = ring_copy(piece, own, landing, d, 0)

    tok_all[my_rows, :] = tokens[...]
    for copy in token_copies:
        copy.wait_recv()
    wide = tok_all[...].astype(f32)
    scale = lax.rsqrt(jnp.mean(wide * wide, axis=1, keepdims=True) + norm_floor)
    normed[...] = (wide * scale * pre_gain[...]).astype(bf16)

    cols = (
        slice(0, lh * dk),
        slice(lh * dk, lh * (dk + dv)),
        slice(lh * (dk + dv), lh * (2 * dk + dv)),
    )
    mine = normed[:, pl.ds(pl.multiple_of(s * depth, depth), depth)]
    for piece, own, landing in pieces:
        acc[:, cols[piece]] = jnp.dot(mine, own[...], preferred_element_type=f32)
    all_normed = normed[...]
    gate_in = jnp.dot(all_normed, w_igate[...], preferred_element_type=f32)
    gate_forget = jnp.dot(all_normed, w_fgate[...], preferred_element_type=f32) + forget_base[...]
    log_forget_all = jnp.minimum(gate_forget, 0.0) - jnp.log1p(jnp.exp(-jnp.abs(gate_forget)))

    for k in range(steps):
        for piece, own, landing in pieces:
            for d in range(2):
                live[piece, d].wait_recv()
                if k + 1 < steps:
                    live[piece, d] = ring_copy(piece, own, landing, d, k + 1)
        if k == steps - 1:
            for d in range(2):
                live[3, d] = ring_copy(3, w_out, out_in, d, 0)
        for d in range(2):
            owner = owner_at(pos - 1 - k) if d == 0 else owner_at(pos + 1 + k)
            part = normed[:, pl.ds(pl.multiple_of(owner * depth + d * half, half), half)]
            for piece, own, landing in pieces:
                acc[:, cols[piece]] += jnp.dot(
                    part, landing[d, k], preferred_element_type=f32
                )

    row_id = lax.broadcasted_iota(jnp.int32, (length, length), 0)
    col_id = lax.broadcasted_iota(jnp.int32, (length, length), 1)
    causal = row_id >= col_id
    head_id = lax.broadcasted_iota(jnp.int32, gate_in.shape, 1)
    keys = (acc[:, cols[0]] * (dk**-0.5)).astype(bf16)
    values = acc[:, cols[1]].astype(bf16)
    queries = acc[:, cols[2]].astype(bf16)
    gates = []
    for j in range(lh):
        pick = head_id == t * lh + j
        in_col = jnp.sum(jnp.where(pick, gate_in, 0.0), axis=1, keepdims=True)
        lf_col = jnp.sum(jnp.where(pick, log_forget_all, 0.0), axis=1, keepdims=True)
        lf_row = jnp.sum(jnp.where(row_id == col_id, lf_col, 0.0), axis=0, keepdims=True)
        in_row = jnp.sum(jnp.where(row_id == col_id, in_col, 0.0), axis=0, keepdims=True)
        b_col = jnp.sum(jnp.where(causal, lf_row, 0.0), axis=1, keepdims=True)
        b_row = jnp.sum(jnp.where(row_id <= col_id, lf_col, 0.0), axis=0, keepdims=True)
        gates.append((in_row, b_col, b_row))
        span = jnp.sum(lf_col, axis=0, keepdims=True)
        write = span - b_col + in_col
        top = jnp.max(write, axis=0, keepdims=True)
        key_scaled = keys[:, j * dk : (j + 1) * dk].astype(f32) * jnp.exp(write - top)
        state_own[j * dk : (j + 1) * dk, :] = jnp.dot(
            key_scaled.T.astype(bf16),
            values[:, j * dv : (j + 1) * dv],
            preferred_element_type=f32,
        ).astype(bf16)
        aux_own[j : j + 1, :] = jnp.broadcast_to(span, (1, dk))
        aux_own[lh + j : lh + j + 1, :] = jnp.broadcast_to(top, (1, dk))
        aux_own[2 * lh + j : 2 * lh + j + 1, :] = jnp.sum(key_scaled, axis=0, keepdims=True)

    for d in range(2):
        live[4, d] = ring_copy(4, state_own, state_in, d, 0)
    aux_live = aux_copy(0)
    intra = []
    for k in range(steps):
        if k < lh:
            in_row, b_col, b_row = gates[k]
            log_pair = jnp.where(causal, b_col - b_row + in_row, lowest_log)
            peak = jnp.max(log_pair, axis=1, keepdims=True)
            q = queries[:, k * dk : (k + 1) * dk]
            weights = dot_nt(q, keys[:, k * dk : (k + 1) * dk]) * jnp.where(
                causal, jnp.exp(log_pair - peak), 0.0
            )
            numer = jnp.dot(
                weights.astype(bf16),
                values[:, k * dv : (k + 1) * dv],
                preferred_element_type=f32,
            )
            intra.append((numer, jnp.sum(weights, axis=1, keepdims=True), peak, q, b_col))
        aux_live.wait_recv()
        if k + 1 < steps:
            aux_live = aux_copy(k + 1)
        for piece, own, landing in ((4, state_own, state_in), (3, w_out, out_in)):
            for d in range(2):
                live[piece, d].wait_recv()
                if k + 1 < steps:
                    live[piece, d] = ring_copy(piece, own, landing, d, k + 1)

    owners = [owner_at(pos - 1 - k) for k in range(steps)]

    def when(flag):
        return flag.astype(jnp.int32).astype(f32)

    for j in range(lh):
        logs = []
        for k in range(steps):
            total = aux_in[k, lh + j : lh + j + 1, :]
            for i in range(steps):
                if i != k:
                    between = when((owners[i] > owners[k]) & (owners[i] < s))
                    total = total + between * aux_in[i, j : j + 1, :]
            before = when(owners[k] < s)
            logs.append((before, before * total + (1.0 - before) * lowest_log))
        entry = functools.reduce(jnp.maximum, [log for _, log in logs])
        mat = jnp.zeros((dk, dv), f32)
        vec = jnp.zeros((1, dk), f32)
        split = (lh * dk) // 2
        d = (j * dk) // split
        base = j * dk - d * split
        for k in range(steps):
            before, log = logs[k]
            weight = before * jnp.exp(log - entry)
            slot = k if d == 0 else steps - 1 - k
            mat = mat + weight[:, :1] * state_in[d, slot, base : base + dk, :].astype(f32)
            vec = vec + weight * aux_in[k, 2 * lh + j : 2 * lh + j + 1, :]
        numer, denom, peak, q, b_col = intra[j]
        carried = b_col + entry[:, :1]
        new_top = jnp.maximum(peak, carried)
        w_intra = jnp.exp(peak - new_top)
        w_carry = jnp.exp(carried - new_top)
        numer = w_intra * numer + w_carry * jnp.dot(
            q, mat.astype(bf16), preferred_element_type=f32
        )
        denom = w_intra * denom + w_carry * jnp.sum(q.astype(f32) * vec, axis=1, keepdims=True)
        hidden = numer / jnp.maximum(jnp.abs(denom), jnp.exp(-new_top))
        gain = head_gain[:, pl.ds(pl.multiple_of((t * lh + j) * dv, dv), dv)]
        heads[:, j * dv : (j + 1) * dv] = (
            hidden
            * lax.rsqrt(jnp.mean(hidden * hidden, axis=1, keepdims=True) + norm_floor)
            * gain
        ).astype(bf16)

    ready = heads[...]
    out_depth = w_out.shape[0]
    out_half = out_depth // 2
    shares[:, pl.ds(pl.multiple_of(s * out_depth, out_depth), out_depth)] = dot_nt(
        ready, w_out[...]
    ).astype(bf16)
    for k in range(steps):
        for d in range(2):
            owner = owner_at(pos - 1 - k) if d == 0 else owner_at(pos + 1 + k)
            at = pl.ds(pl.multiple_of(owner * out_depth + d * out_half, out_half), out_half)
            shares[:, at] = dot_nt(ready, out_in[d, k]).astype(bf16)
    share_copies = []
    for i in range(1, tp):
        peer = lax.rem(t + i, tp)
        copy = pltpu.make_async_remote_copy(
            src_ref=shares.at[pl.ds(pl.multiple_of(peer * rows, rows), rows)],
            dst_ref=shares_in.at[i - 1],
            send_sem=share_send.at[i - 1],
            recv_sem=share_recv.at[i - 1],
            device_id={"tp": peer},
            device_id_type=MESH,
        )
        copy.start()
        copies.append(copy)
        share_copies.append(copy)
    total = shares[my_rows, :].astype(f32)
    for i, copy in enumerate(share_copies):
        copy.wait_recv()
        total = total + shares_in[i].astype(f32)
    out[...] = total.astype(bf16)
    for copy in copies:
        copy.wait_send()


def on_device_ring(
    n,
    tp,
    tokens,
    pre_gain,
    w_query,
    w_key,
    w_value,
    w_igate,
    w_fgate,
    forget_bias,
    gate_drift,
    head_gain,
    w_out,
):
    lh = w_igate.shape[1] // tp
    rows, width = tokens.shape
    length = rows * tp
    steps = n - 1
    dk = w_query.shape[1] // lh
    dv = w_value.shape[1] // lh
    vmem = pl.BlockSpec(memory_space=pltpu.VMEM)

    def landing(a):
        return pltpu.VMEM((2, steps, a.shape[0] // 2, a.shape[1]), bf16)

    aux_rows = -(-3 * lh // 8) * 8
    return pl.pallas_call(
        functools.partial(ring_kernel, n, tp, lh),
        out_shape=jax.ShapeDtypeStruct((rows, w_out.shape[0] * n), bf16),
        in_specs=[vmem] * 10,
        out_specs=vmem,
        scratch_shapes=[
            pltpu.VMEM((length, width), bf16),
            pltpu.VMEM((length, width), bf16),
            landing(w_key),
            landing(w_value),
            landing(w_query),
            landing(w_out),
            pltpu.VMEM((lh * dk, dv), bf16),
            pltpu.VMEM((2, steps, lh * dk // 2, dv), bf16),
            pltpu.VMEM((aux_rows, dk), f32),
            pltpu.VMEM((steps, aux_rows, dk), f32),
            pltpu.VMEM((length, lh * (2 * dk + dv)), f32),
            pltpu.VMEM((length, lh * dv), bf16),
            pltpu.VMEM((length, w_out.shape[0] * n), bf16),
            pltpu.VMEM((tp - 1, rows, w_out.shape[0] * n), bf16),
            pltpu.SemaphoreType.DMA((tp - 1,)),
            pltpu.SemaphoreType.DMA((tp - 1,)),
            pltpu.SemaphoreType.DMA((5, 2, steps)),
            pltpu.SemaphoreType.DMA((5, 2, steps)),
            pltpu.SemaphoreType.DMA((steps,)),
            pltpu.SemaphoreType.DMA((steps,)),
            pltpu.SemaphoreType.DMA((tp - 1,)),
            pltpu.SemaphoreType.DMA((tp - 1,)),
        ],
        compiler_params=pltpu.CompilerParams(collective_id=0, has_side_effects=True),
    )(
        tokens,
        pre_gain.astype(f32)[None, :],
        w_query,
        w_key,
        w_value,
        w_igate,
        w_fgate,
        gate_drift + forget_bias,
        head_gain.astype(f32)[None, :],
        w_out,
    )


def solution(mesh):
    in_specs = (
        P(("sp", "tp"), None),
        P(),
        P("sp", "tp"),
        P("sp", "tp"),
        P("sp", "tp"),
        P(),
        P(),
        P(),
        P("sp", None),
        P(),
        P("sp", "tp"),
    )
    out_specs = P(("sp", "tp"), None)
    body = on_device
    if mesh.shape["sp"] <= ring_limit and mesh.shape["sp"] % 2 == 0:
        body = functools.partial(on_device_ring, mesh.shape["sp"], mesh.shape["tp"])
    return jax.shard_map(
        body, mesh=mesh, in_specs=in_specs, out_specs=out_specs, check_vma=False
    )
```

```python
import functools

import jax
import jax.numpy as jnp
from jax import lax
from jax.experimental import pallas as pl
from jax.experimental.pallas import tpu as pltpu
from jax.sharding import PartitionSpec as P

BLOCK = 64


norm_floor = 0.1
lowest_log = -1e30
highest = lax.Precision.HIGHEST


def prefix(value, axis, combine, identity):
    peers, position = (lax.axis_size(axis), lax.axis_index(axis))
    everything = jax.tree.map(
        lambda part, kind: lax.all_gather(part.astype(kind), axis),
        value,
        jax.tree.map(lambda a: jnp.bfloat16 if a.dtype == jnp.float32 else a.dtype, value),
    )
    start = jax.tree.map(
        lambda part, zero: jnp.broadcast_to(jnp.asarray(zero, part.dtype), part.shape),
        value,
        identity,
    )

    def step(k, before):
        reached = k < position
        new = combine(
            before, jax.tree.map(lambda part, own: part[k].astype(own.dtype), everything, value)
        )
        return jax.tree.map(lambda a, b: jnp.where(reached, a, b), new, before)

    return lax.fori_loop(0, peers, step, start)


def advance(memory, summary):
    old_mat, old_vec, old_top = memory
    span_log, span_top, span_mat, span_vec = summary
    new_top = jnp.maximum(span_log + old_top, span_top)
    kept_part = jnp.exp(span_log + old_top - new_top)
    fresh_part = jnp.exp(span_top - new_top)
    return (
        kept_part[:, None, None] * old_mat + fresh_part[:, None, None] * span_mat,
        kept_part[:, None] * old_vec + fresh_part[:, None] * span_vec,
        new_top,
    )


def prefix_states(initial, summary):

    def stepper(memory, one_block):
        return (advance(memory, one_block), memory)

    return lax.scan(stepper, initial, summary)


def join_devices(earlier, later_part):
    early_log, early_mat, early_vec, early_top = earlier
    late_log, late_mat, late_vec, late_top = later_part
    new_top = jnp.maximum(late_log + early_top, late_top)
    kept_part = jnp.exp(late_log + early_top - new_top)
    fresh_part = jnp.exp(late_top - new_top)
    return (
        early_log + late_log,
        kept_part[:, None, None] * early_mat + fresh_part[:, None, None] * late_mat,
        kept_part[:, None] * early_vec + fresh_part[:, None] * late_vec,
        new_top,
    )


def blend_parts(first_part, second_part):
    numer_first, denom_first, peak_first = first_part
    numer_second, denom_second, peak_second = second_part
    new_top = jnp.maximum(peak_first, peak_second)
    weight_first = jnp.exp(peak_first - new_top)
    weight_second = jnp.exp(peak_second - new_top)
    return (
        weight_first[..., None] * numer_first + weight_second[..., None] * numer_second,
        weight_first * denom_first + weight_second * denom_second,
        new_top,
    )


def on_device(
    tokens,
    pre_gain,
    w_query,
    w_key,
    w_value,
    w_igate,
    w_fgate,
    forget_bias,
    gate_drift,
    head_gain,
    w_out,
):
    tp_size = lax.axis_size("tp")
    head_count = w_igate.shape[1]
    local_heads = head_count // tp_size
    first_head = lax.axis_index("tp") * local_heads
    key_width = w_query.shape[1] // local_heads
    value_width = w_value.shape[1] // local_heads
    token_wide = tokens.astype(jnp.float32)
    scaled = token_wide * lax.rsqrt(
        jnp.mean(token_wide * token_wide, axis=1, keepdims=True) + norm_floor
    )
    normed = (scaled * pre_gain.astype(jnp.float32)).astype(jnp.bfloat16)
    gate_cols = jnp.concatenate(
        [
            lax.dynamic_slice_in_dim(w_igate, first_head, local_heads, 1),
            lax.dynamic_slice_in_dim(w_fgate, first_head, local_heads, 1),
        ],
        axis=1,
    )
    key_scale = key_width ** (-0.5)
    wq_full, wk_full, wv_full = (
        lax.all_gather(w_query, "sp", axis=0, tiled=True),
        lax.all_gather(w_key, "sp", axis=0, tiled=True),
        lax.all_gather(w_value, "sp", axis=0, tiled=True),
    )
    row_piece = lax.all_gather(normed, "tp", axis=0, tiled=True)
    queries_part = jnp.dot(row_piece, wq_full, preferred_element_type=jnp.float32).astype(
        jnp.bfloat16
    )
    keys_part = (
        jnp.dot(row_piece, wk_full, preferred_element_type=jnp.float32) * key_scale
    ).astype(jnp.bfloat16)
    values_part = jnp.dot(row_piece, wv_full, preferred_element_type=jnp.float32).astype(
        jnp.bfloat16
    )
    gate_part = jnp.dot(row_piece, gate_cols, preferred_element_type=jnp.float32)
    group_len = queries_part.shape[0]
    blocks = group_len // BLOCK
    log_input = gate_part[:, :local_heads]
    forget_pre = gate_part[:, local_heads:] + lax.dynamic_slice_in_dim(
        forget_bias, first_head, local_heads, 0
    )
    log_forget = jax.nn.log_sigmoid(
        forget_pre + lax.dynamic_slice_in_dim(gate_drift, first_head, local_heads, 1)
    )
    query_blk = queries_part.reshape(blocks, BLOCK, local_heads, key_width)
    key_blk = keys_part.reshape(blocks, BLOCK, local_heads, key_width)
    value_blk = values_part.reshape(blocks, BLOCK, local_heads, value_width)
    input_blk = log_input.reshape(blocks, BLOCK, local_heads).transpose(0, 2, 1)
    forget_blk = log_forget.reshape(blocks, BLOCK, local_heads).transpose(0, 2, 1)
    within = jnp.cumsum(forget_blk, axis=2)
    causal = jnp.arange(BLOCK)[:, None] >= jnp.arange(BLOCK)[None, :]
    log_pair = jnp.where(
        causal, within[..., :, None] - within[..., None, :] + input_blk[..., None, :], -jnp.inf
    )
    peak_intra = jnp.max(log_pair, axis=3)
    scores = jnp.einsum("nshd,nrhd->nhsr", query_blk, key_blk, preferred_element_type=jnp.float32)
    weights = scores * jnp.exp(log_pair - peak_intra[..., None])
    numer_intra = jnp.einsum(
        "nhsr,nrhv->nhsv",
        weights.astype(jnp.bfloat16),
        value_blk,
        preferred_element_type=jnp.float32,
    )
    denom_intra = jnp.sum(weights, axis=3)
    span_log = within[..., -1]
    log_write = span_log[..., None] - within + input_blk
    span_top = jnp.max(log_write, axis=2)
    write_scale = jnp.exp(log_write - span_top[..., None])
    key_scaled = key_blk.astype(jnp.float32) * write_scale.transpose(0, 2, 1)[..., None]
    value_wide = value_blk.astype(jnp.float32)
    span_mat = jnp.einsum("nrhv,nrhd->nhvd", value_wide, key_scaled, precision=highest)
    span_vec = jnp.sum(key_scaled, axis=1)
    summary = (span_log, span_top, span_mat, span_vec)
    empty_state = (
        jnp.zeros((local_heads, value_width, key_width), jnp.float32),
        jnp.zeros((local_heads, key_width), jnp.float32),
        jnp.full((local_heads,), lowest_log, jnp.float32),
    )
    local_end, local_starts = prefix_states(empty_state, summary)
    device_summary = (jnp.sum(span_log, axis=0),) + local_end
    identity_all = (jnp.zeros((local_heads,), jnp.float32),) + empty_state
    incoming = prefix(device_summary, "sp", join_devices, identity_all)
    query_wide = query_blk.astype(jnp.float32)
    intra_part = (numer_intra, denom_intra, peak_intra)
    start_mat, start_vec, start_top = local_starts
    local_part = (
        jnp.einsum("nhvd,nshd->nhsv", start_mat, query_wide, precision=highest),
        jnp.einsum("nhd,nshd->nhs", start_vec, query_wide, precision=highest),
        within + start_top[..., None],
    )
    numerator, denominator, peak_log = blend_parts(local_part, intra_part)
    entry_log, entry_mat, entry_vec, entry_top = incoming
    before_log = jnp.concatenate(
        [jnp.zeros((1, local_heads), jnp.float32), jnp.cumsum(span_log, axis=0)[:-1]], axis=0
    )
    from_left = (
        jnp.einsum("hvd,nshd->nhsv", entry_mat, query_wide, precision=highest),
        jnp.einsum("hd,nshd->nhs", entry_vec, query_wide, precision=highest),
        within + (before_log + entry_top[None, :])[..., None],
    )
    numerator, denominator, peak_log = blend_parts((numerator, denominator, peak_log), from_left)
    hidden = numerator / jnp.maximum(jnp.abs(denominator), jnp.exp(-peak_log))[..., None]
    hidden = hidden.transpose(0, 2, 1, 3).reshape(group_len, local_heads, value_width)
    head_gains = lax.dynamic_slice_in_dim(
        head_gain, first_head * value_width, local_heads * value_width, 0
    )
    head_gains = head_gains.astype(jnp.float32).reshape(local_heads, value_width)
    normed_heads = (
        hidden
        * lax.rsqrt(jnp.mean(hidden * hidden, axis=2, keepdims=True) + norm_floor)
        * head_gains
    )
    normed_heads = normed_heads.astype(jnp.bfloat16).reshape(group_len, local_heads * value_width)
    out_slab = lax.all_gather(w_out, "sp", axis=0, tiled=True)
    return lax.psum_scatter(
        lax.dot_general(
            normed_heads, out_slab, (((1,), (1,)), ((), ())), preferred_element_type=jnp.float32
        ).astype(jnp.bfloat16),
        "tp",
        scatter_dimension=0,
        tiled=True,
    )


ring_limit = 16
drift_span = 128
MESH = pl.DeviceIdType.MESH
f32 = jnp.float32
bf16 = jnp.bfloat16


def dot_nt(a, b):
    return lax.dot_general(a, b, (((1,), (1,)), ((), ())), preferred_element_type=f32)


def when(flag):
    return flag.astype(jnp.int32).astype(f32)


def square_kernel(
    n,
    tp,
    tokens,
    pre_gain,
    w_query,
    w_key,
    w_value,
    w_igate,
    w_fgate,
    drift,
    head_gain,
    w_out,
    out,
    tok_all,
    drift_in,
    normed,
    own_key,
    own_value,
    own_query,
    own_out,
    key_in,
    value_in,
    query_in,
    out_in,
    state_own,
    state_in,
    aux_own,
    aux_in,
    acc,
    heads,
    shares,
    pair_in,
    pair_sum,
    shares_in,
    tok_send,
    tok_recv,
    drift_send,
    drift_recv,
    near_send,
    near_recv,
    first_send,
    first_recv,
    ring_send,
    ring_recv,
    state_send,
    state_recv,
    aux_send,
    aux_recv,
    pair_send,
    pair_recv,
    share_send,
    share_recv,
):
    s = lax.axis_index("sp")
    t = lax.axis_index("tp")
    q = n // 2
    steps = q - 1
    zh = s // q
    r = s % q
    y = t // 2
    c = t % 2
    near = 2 * y + 1 - c
    head = 2 * (2 * y + zh) + c
    rows = tokens.shape[0]
    span_rows = rows * tp
    length = 2 * span_rows
    dk = w_query.shape[1] // 2
    dv = w_value.shape[1] // 2
    depth = w_query.shape[0]
    half = depth // 2
    half_ring = q // 2
    odd = r % 2
    pos = odd * (q - 1) + (1 - 2 * odd) * (r // 2)

    def owner_at(p):
        p = lax.rem(p + 2 * q, q)
        far = p // half_ring
        return far * (2 * (q - 1 - p) + 1) + (1 - far) * 2 * p

    targets = (zh * q + owner_at(pos + 1), zh * q + owner_at(pos - 1))

    barrier = pltpu.get_barrier_semaphore()
    me = s * tp + t
    for i in range(1, n * tp):
        other = lax.rem(me + i, n * tp)
        pl.semaphore_signal(
            barrier,
            inc=1,
            device_id={"sp": other // tp, "tp": lax.rem(other, tp)},
            device_id_type=MESH,
        )
    pl.semaphore_wait(barrier, n * tp - 1)

    copies = []
    guarded = []

    def remote(source, target, send, recv, sp_at, tp_at):
        return pltpu.make_async_remote_copy(
            src_ref=source,
            dst_ref=target,
            send_sem=send,
            recv_sem=recv,
            device_id={"sp": sp_at, "tp": tp_at},
            device_id_type=MESH,
        )

    def send(*args):
        copy = remote(*args)
        copy.start()
        copies.append(copy)
        return copy

    def send_or_keep(source, target, send_sem, recv_sem, sp_at, tp_at):
        away = (sp_at != s) | (tp_at != t)
        copy = remote(source, target, send_sem, recv_sem, sp_at, tp_at)

        @pl.when(away)
        def _():
            copy.start()

        @pl.when(jnp.logical_not(away))
        def _():
            pltpu.make_async_copy(source, target, recv_sem).start()

        guarded.append((away, copy))
        return copy

    def arrived(target, sem):
        pltpu.make_async_copy(target, target, sem).wait()

    half_tp = tp // 2
    x = s % 2
    row_at = pl.ds(pl.multiple_of(x * span_rows + t * rows, rows), rows)
    for g in range(2):
        for yy in range(half_tp):
            to_s, to_t = g * q + s // 2, 2 * yy + c
            send_or_keep(
                tokens,
                tok_all.at[row_at],
                tok_send.at[g, yy],
                tok_recv.at[x, y],
                to_s,
                to_t,
            )
            send_or_keep(
                drift,
                drift_in.at[x, y],
                drift_send.at[g, yy],
                drift_recv.at[x, y],
                to_s,
                to_t,
            )

    pieces = (
        (0, w_key, own_key, key_in),
        (1, w_value, own_value, value_in),
        (2, w_query, own_query, query_in),
        (3, w_out, own_out, out_in),
    )
    stays = zh == c
    first = []
    for p, own, stage, _ in pieces:
        width = own.shape[1] // 2
        for g in range(2):
            mine = own.at[:, pl.ds(g * width, width)]
            keep = stays & (c == g)
            block = (zh + c) % 2
            copy = remote(
                mine,
                stage.at[block],
                first_send.at[g, p],
                first_recv.at[block, p],
                c * q + r,
                2 * y + g,
            )

            @pl.when(jnp.logical_not(keep))
            def _():
                copy.start()

            @pl.when(keep)
            def _():
                pltpu.make_async_copy(mine, stage.at[0], first_recv.at[0, p]).start()

            guarded.append((jnp.logical_not(keep), copy))

    def ring_copy(p, block, d, k):
        _, _, stage, landing = pieces[p]
        size = stage.shape[1] // 2
        source = (
            stage.at[block, pl.ds(d * size, size)] if k == 0 else landing.at[block, d, k - 1]
        )
        return send(
            source,
            landing.at[block, d, k],
            ring_send.at[p, block, d, k],
            ring_recv.at[p, block, d, k],
            targets[d],
            t,
        )

    live = {}

    def ring_start(p, block):
        arrived(pieces[p][2].at[block], first_recv.at[block, p])
        for d in range(2):
            live[p, block, d] = ring_copy(p, block, d, 0)

    def ring_step(p, block, k):
        for d in range(2):
            live[p, block, d].wait_recv()
            if k + 1 < steps:
                live[p, block, d] = ring_copy(p, block, d, k + 1)

    for p in range(3):
        ring_start(p, 0)

    for xx in range(2):
        for yy in range(half_tp):
            at = pl.ds(
                pl.multiple_of(xx * span_rows + (2 * yy + c) * rows, rows), rows
            )
            arrived(tok_all.at[at], tok_recv.at[xx, yy])
            arrived(drift_in.at[xx, yy], drift_recv.at[xx, yy])
            send(
                tok_all.at[at],
                tok_all.at[at],
                near_send.at[xx, yy],
                near_recv.at[xx, yy],
                s,
                near,
            )
    for xx in range(2):
        for yy in range(half_tp):
            at = pl.ds(
                pl.multiple_of(xx * span_rows + (2 * yy + 1 - c) * rows, rows), rows
            )
            arrived(tok_all.at[at], near_recv.at[xx, yy])
    wide = tok_all[...].astype(f32)
    scale = lax.rsqrt(jnp.mean(wide * wide, axis=1, keepdims=True) + norm_floor)
    normed[...] = (wide * scale * pre_gain[...]).astype(bf16)

    cols = (slice(0, dk), slice(dk, dk + dv), slice(dk + dv, 2 * dk + dv))

    def origin(block, owner):
        return (zh if block == 0 else 1 - zh) * q + owner

    def own_product(block, fresh):
        at = pl.ds(pl.multiple_of(origin(block, r) * depth, depth), depth)
        part = normed[:, at]
        for p in range(3):
            product = jnp.dot(part, pieces[p][2][block], preferred_element_type=f32)
            acc[:, cols[p]] = product if fresh else acc[:, cols[p]] + product

    def step_product(block, k):
        for d in range(2):
            owner = owner_at(pos - 1 - k) if d == 0 else owner_at(pos + 1 + k)
            at = pl.ds(
                pl.multiple_of(origin(block, owner) * depth + d * half, half), half
            )
            part = normed[:, at]
            for p in range(3):
                acc[:, cols[p]] += jnp.dot(
                    part, pieces[p][3][block, d, k], preferred_element_type=f32
                )

    own_product(0, True)
    for k in range(steps):
        for p in range(3):
            ring_step(p, 0, k)
        if k == steps - 2:
            for p in range(3):
                ring_start(p, 1)
        step_product(0, k)
    ring_start(3, 0)

    all_normed = normed[...]
    gate_in = jnp.dot(all_normed, w_igate[...], preferred_element_type=f32)
    gate_forget = jnp.dot(all_normed, w_fgate[...], preferred_element_type=f32)
    row_id = lax.broadcasted_iota(jnp.int32, (length, length), 0)
    col_id = lax.broadcasted_iota(jnp.int32, (length, length), 1)
    causal = row_id >= col_id
    pick = lax.broadcasted_iota(jnp.int32, gate_in.shape, 1) == head
    late = lax.broadcasted_iota(jnp.int32, gate_in.shape, 0) >= span_rows
    heads_all = gate_in.shape[1]
    offset = jnp.where(
        late, drift_in[1, 0, 0:1, :heads_all], drift_in[0, 0, 0:1, :heads_all]
    )
    forget_pre = gate_forget + offset
    log_forget = jnp.minimum(forget_pre, 0.0) - jnp.log1p(jnp.exp(-jnp.abs(forget_pre)))
    in_col = jnp.sum(jnp.where(pick, gate_in, 0.0), axis=1, keepdims=True)
    lf_col = jnp.sum(jnp.where(pick, log_forget, 0.0), axis=1, keepdims=True)
    lf_row = jnp.sum(jnp.where(row_id == col_id, lf_col, 0.0), axis=0, keepdims=True)
    in_row = jnp.sum(jnp.where(row_id == col_id, in_col, 0.0), axis=0, keepdims=True)
    b_col = jnp.sum(jnp.where(causal, lf_row, 0.0), axis=1, keepdims=True)
    b_row = jnp.sum(jnp.where(row_id <= col_id, lf_col, 0.0), axis=0, keepdims=True)
    span = jnp.sum(lf_col, axis=0, keepdims=True)
    write = span - b_col + in_col
    top = jnp.max(write, axis=0, keepdims=True)
    write_scale = jnp.exp(write - top)
    log_pair = jnp.where(causal, b_col - b_row + in_row, lowest_log)
    peak = jnp.max(log_pair, axis=1, keepdims=True)
    decay = jnp.where(causal, jnp.exp(log_pair - peak), 0.0)

    own_product(1, False)
    for k in range(steps):
        for p in range(3):
            ring_step(p, 1, k)
        step_product(1, k)
    ring_start(3, 1)

    keys = (acc[:, cols[0]] * (dk**-0.5)).astype(bf16)
    values = acc[:, cols[1]].astype(bf16)
    queries = acc[:, cols[2]].astype(bf16)
    key_scaled = keys.astype(f32) * write_scale
    state_own[...] = jnp.dot(
        key_scaled.T.astype(bf16), values, preferred_element_type=f32
    ).astype(bf16)
    aux_own[0:1, :] = jnp.broadcast_to(span, (1, dk))
    aux_own[1:2, :] = jnp.broadcast_to(top, (1, dk))
    aux_own[2:3, :] = jnp.sum(key_scaled, axis=0, keepdims=True)
    aux_own[3:, :] = jnp.zeros((aux_own.shape[0] - 3, dk), f32)
    state_copies = []
    for i in range(1, q):
        peer = zh * q + lax.rem(r + i, q)
        state_copies.append(
            (
                send(
                    state_own,
                    state_in.at[i - 1],
                    state_send.at[i - 1],
                    state_recv.at[i - 1],
                    peer,
                    t,
                ),
                send(
                    aux_own,
                    aux_in.at[i - 1],
                    aux_send.at[i - 1],
                    aux_recv.at[i - 1],
                    peer,
                    t,
                ),
            )
        )
    weights = dot_nt(queries, keys) * decay
    numer = jnp.dot(weights.astype(bf16), values, preferred_element_type=f32)
    denom = jnp.sum(weights, axis=1, keepdims=True)
    ring_step(3, 0, 0)
    ring_step(3, 1, 0)

    for pair in state_copies:
        for copy in pair:
            copy.wait_recv()
    owners = [lax.rem(r - i + q, q) for i in range(1, q)]
    logs = []
    for k in range(steps):
        total = aux_in[k, 1:2, :]
        for i in range(steps):
            if i != k:
                between = when((owners[i] > owners[k]) & (owners[i] < r))
                total = total + between * aux_in[i, 0:1, :]
        before = when(owners[k] < r)
        logs.append((before, before * total + (1.0 - before) * lowest_log))
    entry = functools.reduce(jnp.maximum, [log for _, log in logs])
    mat = jnp.zeros((dk, dv), f32)
    vec = jnp.zeros((1, dk), f32)
    for k in range(steps):
        before, log = logs[k]
        weight = before * jnp.exp(log - entry)
        mat = mat + weight[:, :1] * state_in[k].astype(f32)
        vec = vec + weight * aux_in[k, 2:3, :]
    carried = b_col + entry[:, :1]
    new_top = jnp.maximum(peak, carried)
    w_intra = jnp.exp(peak - new_top)
    w_carry = jnp.exp(carried - new_top)
    numer = w_intra * numer + w_carry * jnp.dot(
        queries, mat.astype(bf16), preferred_element_type=f32
    )
    denom = w_intra * denom + w_carry * jnp.sum(
        queries.astype(f32) * vec, axis=1, keepdims=True
    )
    hidden = numer / jnp.maximum(jnp.abs(denom), jnp.exp(-new_top))
    gain = head_gain[:, pl.ds(pl.multiple_of(head * dv, dv), dv)]
    heads[...] = (
        hidden
        * lax.rsqrt(jnp.mean(hidden * hidden, axis=1, keepdims=True) + norm_floor)
        * gain
    ).astype(bf16)

    ready = heads[...]
    e_depth = w_out.shape[0]
    e_half = e_depth // 2
    for block in range(2):
        at = pl.ds(pl.multiple_of(origin(block, r) * e_depth, e_depth), e_depth)
        shares[:, at] = dot_nt(ready, own_out[block]).astype(bf16)
    for k in range(steps):
        for block in range(2):
            if k > 0:
                ring_step(3, block, k)
            for d in range(2):
                owner = owner_at(pos - 1 - k) if d == 0 else owner_at(pos + 1 + k)
                at = pl.ds(
                    pl.multiple_of(origin(block, owner) * e_depth + d * e_half, e_half),
                    e_half,
                )
                shares[:, at] = dot_nt(ready, out_in[block, d, k]).astype(bf16)

    theirs = pl.ds(pl.multiple_of((1 - c) * span_rows, span_rows), span_rows)
    pair = send(
        shares.at[theirs], pair_in, pair_send.at[0], pair_recv.at[0], s, near
    )
    pair.wait_recv()
    kept = pl.ds(pl.multiple_of(c * span_rows, span_rows), span_rows)
    pair_sum[...] = (shares[kept, :].astype(f32) + pair_in[...].astype(f32)).astype(bf16)
    for to_t in range(tp):
        send_or_keep(
            pair_sum.at[pl.ds(to_t * rows, rows)],
            shares_in.at[zh, y],
            share_send.at[to_t],
            share_recv.at[zh, y],
            2 * r + c,
            to_t,
        )
    total = jnp.zeros(out.shape, f32)
    for g in range(2):
        for yy in range(half_tp):
            arrived(shares_in.at[g, yy], share_recv.at[g, yy])
            total = total + shares_in[g, yy].astype(f32)
    out[...] = total.astype(bf16)
    for copy in copies:
        copy.wait_send()
    for away, copy in guarded:

        @pl.when(away)
        def _():
            copy.wait_send()


def on_device_ring(
    n,
    tp,
    tokens,
    pre_gain,
    w_query,
    w_key,
    w_value,
    w_igate,
    w_fgate,
    forget_bias,
    gate_drift,
    head_gain,
    w_out,
):
    heads = w_igate.shape[1]
    if heads != 2 * tp or gate_drift.shape[0] > drift_span:
        return on_device(
            tokens,
            pre_gain,
            w_query,
            w_key,
            w_value,
            w_igate,
            w_fgate,
            forget_bias,
            gate_drift,
            head_gain,
            w_out,
        )
    rows, width = tokens.shape
    length = 2 * rows * tp
    q = n // 2
    steps = q - 1
    half_tp = tp // 2
    dk = w_query.shape[1] // 2
    dv = w_value.shape[1] // 2
    features = w_out.shape[0] * n
    vmem = pl.BlockSpec(memory_space=pltpu.VMEM)
    dma = pltpu.SemaphoreType.DMA
    weights = (w_key, w_value, w_query, w_out)
    base = gate_drift[:8] + forget_bias
    base = jnp.pad(base, ((0, 0), (0, 128 - heads)))
    return pl.pallas_call(
        functools.partial(square_kernel, n, tp),
        out_shape=jax.ShapeDtypeStruct((rows, features), bf16),
        in_specs=[vmem] * 10,
        out_specs=vmem,
        scratch_shapes=[
            pltpu.VMEM((length, width), bf16),
            pltpu.VMEM((2, half_tp, 8, 128), f32),
            pltpu.VMEM((length, width), bf16),
            *[pltpu.VMEM((2, w.shape[0], w.shape[1] // 2), bf16) for w in weights],
            *[
                pltpu.VMEM((2, 2, steps, w.shape[0] // 2, w.shape[1] // 2), bf16)
                for w in weights
            ],
            pltpu.VMEM((dk, dv), bf16),
            pltpu.VMEM((steps, dk, dv), bf16),
            pltpu.VMEM((8, dk), f32),
            pltpu.VMEM((steps, 8, dk), f32),
            pltpu.VMEM((length, 2 * dk + dv), f32),
            pltpu.VMEM((length, dv), bf16),
            pltpu.VMEM((length, features), bf16),
            pltpu.VMEM((length // 2, features), bf16),
            pltpu.VMEM((length // 2, features), bf16),
            pltpu.VMEM((2, half_tp, rows, features), bf16),
            dma((2, half_tp)),
            dma((2, half_tp)),
            dma((2, half_tp)),
            dma((2, half_tp)),
            dma((2, half_tp)),
            dma((2, half_tp)),
            dma((2, 4)),
            dma((2, 4)),
            dma((4, 2, 2, steps)),
            dma((4, 2, 2, steps)),
            dma((steps,)),
            dma((steps,)),
            dma((steps,)),
            dma((steps,)),
            dma((1,)),
            dma((1,)),
            dma((tp,)),
            dma((2, half_tp)),
        ],
        compiler_params=pltpu.CompilerParams(collective_id=0, has_side_effects=True),
    )(
        tokens,
        pre_gain.astype(f32)[None, :],
        w_query,
        w_key,
        w_value,
        w_igate,
        w_fgate,
        base,
        head_gain.astype(f32)[None, :],
        w_out,
    )


def solution(mesh):
    in_specs = (
        P(("sp", "tp"), None),
        P(),
        P("sp", "tp"),
        P("sp", "tp"),
        P("sp", "tp"),
        P(),
        P(),
        P(),
        P("sp", None),
        P(),
        P("sp", "tp"),
    )
    out_specs = P(("sp", "tp"), None)
    body = on_device
    if mesh.shape["sp"] <= ring_limit and mesh.shape["sp"] % 4 == 0 and mesh.shape["tp"] % 2 == 0:
        body = functools.partial(on_device_ring, mesh.shape["sp"], mesh.shape["tp"])
    return jax.shard_map(
        body, mesh=mesh, in_specs=in_specs, out_specs=out_specs, check_vma=False
    )
```

```python
import functools

import jax
import jax.numpy as jnp
from jax import lax
from jax.experimental import pallas as pl
from jax.experimental.pallas import tpu as pltpu
from jax.sharding import PartitionSpec as P

BLOCK = 64


norm_floor = 0.1
lowest_log = -1e30
highest = lax.Precision.HIGHEST


def prefix(value, axis, combine, identity):
    peers, position = (lax.axis_size(axis), lax.axis_index(axis))
    everything = jax.tree.map(
        lambda part, kind: lax.all_gather(part.astype(kind), axis),
        value,
        jax.tree.map(lambda a: jnp.bfloat16 if a.dtype == jnp.float32 else a.dtype, value),
    )
    start = jax.tree.map(
        lambda part, zero: jnp.broadcast_to(jnp.asarray(zero, part.dtype), part.shape),
        value,
        identity,
    )

    def step(k, before):
        reached = k < position
        new = combine(
            before, jax.tree.map(lambda part, own: part[k].astype(own.dtype), everything, value)
        )
        return jax.tree.map(lambda a, b: jnp.where(reached, a, b), new, before)

    return lax.fori_loop(0, peers, step, start)


def advance(memory, summary):
    old_mat, old_vec, old_top = memory
    span_log, span_top, span_mat, span_vec = summary
    new_top = jnp.maximum(span_log + old_top, span_top)
    kept_part = jnp.exp(span_log + old_top - new_top)
    fresh_part = jnp.exp(span_top - new_top)
    return (
        kept_part[:, None, None] * old_mat + fresh_part[:, None, None] * span_mat,
        kept_part[:, None] * old_vec + fresh_part[:, None] * span_vec,
        new_top,
    )


def prefix_states(initial, summary):

    def stepper(memory, one_block):
        return (advance(memory, one_block), memory)

    return lax.scan(stepper, initial, summary)


def join_devices(earlier, later_part):
    early_log, early_mat, early_vec, early_top = earlier
    late_log, late_mat, late_vec, late_top = later_part
    new_top = jnp.maximum(late_log + early_top, late_top)
    kept_part = jnp.exp(late_log + early_top - new_top)
    fresh_part = jnp.exp(late_top - new_top)
    return (
        early_log + late_log,
        kept_part[:, None, None] * early_mat + fresh_part[:, None, None] * late_mat,
        kept_part[:, None] * early_vec + fresh_part[:, None] * late_vec,
        new_top,
    )


def blend_parts(first_part, second_part):
    numer_first, denom_first, peak_first = first_part
    numer_second, denom_second, peak_second = second_part
    new_top = jnp.maximum(peak_first, peak_second)
    weight_first = jnp.exp(peak_first - new_top)
    weight_second = jnp.exp(peak_second - new_top)
    return (
        weight_first[..., None] * numer_first + weight_second[..., None] * numer_second,
        weight_first * denom_first + weight_second * denom_second,
        new_top,
    )


def on_device(
    tokens,
    pre_gain,
    w_query,
    w_key,
    w_value,
    w_igate,
    w_fgate,
    forget_bias,
    gate_drift,
    head_gain,
    w_out,
):
    tp_size = lax.axis_size("tp")
    head_count = w_igate.shape[1]
    local_heads = head_count // tp_size
    first_head = lax.axis_index("tp") * local_heads
    key_width = w_query.shape[1] // local_heads
    value_width = w_value.shape[1] // local_heads
    token_wide = tokens.astype(jnp.float32)
    scaled = token_wide * lax.rsqrt(
        jnp.mean(token_wide * token_wide, axis=1, keepdims=True) + norm_floor
    )
    normed = (scaled * pre_gain.astype(jnp.float32)).astype(jnp.bfloat16)
    gate_cols = jnp.concatenate(
        [
            lax.dynamic_slice_in_dim(w_igate, first_head, local_heads, 1),
            lax.dynamic_slice_in_dim(w_fgate, first_head, local_heads, 1),
        ],
        axis=1,
    )
    key_scale = key_width ** (-0.5)
    wq_full, wk_full, wv_full = (
        lax.all_gather(w_query, "sp", axis=0, tiled=True),
        lax.all_gather(w_key, "sp", axis=0, tiled=True),
        lax.all_gather(w_value, "sp", axis=0, tiled=True),
    )
    row_piece = lax.all_gather(normed, "tp", axis=0, tiled=True)
    queries_part = jnp.dot(row_piece, wq_full, preferred_element_type=jnp.float32).astype(
        jnp.bfloat16
    )
    keys_part = (
        jnp.dot(row_piece, wk_full, preferred_element_type=jnp.float32) * key_scale
    ).astype(jnp.bfloat16)
    values_part = jnp.dot(row_piece, wv_full, preferred_element_type=jnp.float32).astype(
        jnp.bfloat16
    )
    gate_part = jnp.dot(row_piece, gate_cols, preferred_element_type=jnp.float32)
    group_len = queries_part.shape[0]
    blocks = group_len // BLOCK
    log_input = gate_part[:, :local_heads]
    forget_pre = gate_part[:, local_heads:] + lax.dynamic_slice_in_dim(
        forget_bias, first_head, local_heads, 0
    )
    log_forget = jax.nn.log_sigmoid(
        forget_pre + lax.dynamic_slice_in_dim(gate_drift, first_head, local_heads, 1)
    )
    query_blk = queries_part.reshape(blocks, BLOCK, local_heads, key_width)
    key_blk = keys_part.reshape(blocks, BLOCK, local_heads, key_width)
    value_blk = values_part.reshape(blocks, BLOCK, local_heads, value_width)
    input_blk = log_input.reshape(blocks, BLOCK, local_heads).transpose(0, 2, 1)
    forget_blk = log_forget.reshape(blocks, BLOCK, local_heads).transpose(0, 2, 1)
    within = jnp.cumsum(forget_blk, axis=2)
    causal = jnp.arange(BLOCK)[:, None] >= jnp.arange(BLOCK)[None, :]
    log_pair = jnp.where(
        causal, within[..., :, None] - within[..., None, :] + input_blk[..., None, :], -jnp.inf
    )
    peak_intra = jnp.max(log_pair, axis=3)
    scores = jnp.einsum("nshd,nrhd->nhsr", query_blk, key_blk, preferred_element_type=jnp.float32)
    weights = scores * jnp.exp(log_pair - peak_intra[..., None])
    numer_intra = jnp.einsum(
        "nhsr,nrhv->nhsv",
        weights.astype(jnp.bfloat16),
        value_blk,
        preferred_element_type=jnp.float32,
    )
    denom_intra = jnp.sum(weights, axis=3)
    span_log = within[..., -1]
    log_write = span_log[..., None] - within + input_blk
    span_top = jnp.max(log_write, axis=2)
    write_scale = jnp.exp(log_write - span_top[..., None])
    key_scaled = key_blk.astype(jnp.float32) * write_scale.transpose(0, 2, 1)[..., None]
    value_wide = value_blk.astype(jnp.float32)
    span_mat = jnp.einsum("nrhv,nrhd->nhvd", value_wide, key_scaled, precision=highest)
    span_vec = jnp.sum(key_scaled, axis=1)
    summary = (span_log, span_top, span_mat, span_vec)
    empty_state = (
        jnp.zeros((local_heads, value_width, key_width), jnp.float32),
        jnp.zeros((local_heads, key_width), jnp.float32),
        jnp.full((local_heads,), lowest_log, jnp.float32),
    )
    local_end, local_starts = prefix_states(empty_state, summary)
    device_summary = (jnp.sum(span_log, axis=0),) + local_end
    identity_all = (jnp.zeros((local_heads,), jnp.float32),) + empty_state
    incoming = prefix(device_summary, "sp", join_devices, identity_all)
    query_wide = query_blk.astype(jnp.float32)
    intra_part = (numer_intra, denom_intra, peak_intra)
    start_mat, start_vec, start_top = local_starts
    local_part = (
        jnp.einsum("nhvd,nshd->nhsv", start_mat, query_wide, precision=highest),
        jnp.einsum("nhd,nshd->nhs", start_vec, query_wide, precision=highest),
        within + start_top[..., None],
    )
    numerator, denominator, peak_log = blend_parts(local_part, intra_part)
    entry_log, entry_mat, entry_vec, entry_top = incoming
    before_log = jnp.concatenate(
        [jnp.zeros((1, local_heads), jnp.float32), jnp.cumsum(span_log, axis=0)[:-1]], axis=0
    )
    from_left = (
        jnp.einsum("hvd,nshd->nhsv", entry_mat, query_wide, precision=highest),
        jnp.einsum("hd,nshd->nhs", entry_vec, query_wide, precision=highest),
        within + (before_log + entry_top[None, :])[..., None],
    )
    numerator, denominator, peak_log = blend_parts((numerator, denominator, peak_log), from_left)
    hidden = numerator / jnp.maximum(jnp.abs(denominator), jnp.exp(-peak_log))[..., None]
    hidden = hidden.transpose(0, 2, 1, 3).reshape(group_len, local_heads, value_width)
    head_gains = lax.dynamic_slice_in_dim(
        head_gain, first_head * value_width, local_heads * value_width, 0
    )
    head_gains = head_gains.astype(jnp.float32).reshape(local_heads, value_width)
    normed_heads = (
        hidden
        * lax.rsqrt(jnp.mean(hidden * hidden, axis=2, keepdims=True) + norm_floor)
        * head_gains
    )
    normed_heads = normed_heads.astype(jnp.bfloat16).reshape(group_len, local_heads * value_width)
    out_slab = lax.all_gather(w_out, "sp", axis=0, tiled=True)
    return lax.psum_scatter(
        lax.dot_general(
            normed_heads, out_slab, (((1,), (1,)), ((), ())), preferred_element_type=jnp.float32
        ).astype(jnp.bfloat16),
        "tp",
        scatter_dimension=0,
        tiled=True,
    )


ring_limit = 16
drift_span = 128
MESH = pl.DeviceIdType.MESH
f32 = jnp.float32
bf16 = jnp.bfloat16


def dot_nt(a, b):
    return lax.dot_general(a, b, (((1,), (1,)), ((), ())), preferred_element_type=f32)


def when(flag):
    return flag.astype(jnp.int32).astype(f32)


def square_kernel(
    n,
    tp,
    tokens,
    pre_gain,
    w_query,
    w_key,
    w_value,
    w_igate,
    w_fgate,
    forget_bias,
    drift,
    head_gain,
    w_out,
    out,
    tok_all,
    drift_in,
    normed,
    own_key,
    own_value,
    own_query,
    own_out,
    key_in,
    value_in,
    query_in,
    out_in,
    state_own,
    state_in,
    aux_own,
    aux_in,
    acc,
    heads,
    shares,
    pair_in,
    pair_sum,
    shares_in,
    tok_send,
    tok_recv,
    drift_send,
    drift_recv,
    near_send,
    near_recv,
    first_sems,
    first_recv,
    ring_send,
    ring_recv,
    state_send,
    state_recv,
    aux_send,
    aux_recv,
    pair_send,
    pair_recv,
    share_send,
    share_recv,
):
    s = lax.axis_index("sp")
    t = lax.axis_index("tp")
    q = n // 2
    steps = q - 1
    zh = s // q
    r = s % q
    y = t // 2
    c = t % 2
    near = 2 * y + 1 - c
    head = 2 * (2 * y + zh) + c
    rows = tokens.shape[0]
    span_rows = rows * tp
    length = 2 * span_rows
    dk = w_query.shape[1] // 2
    dv = w_value.shape[1] // 2
    depth = w_query.shape[0]
    half = depth // 2
    half_ring = q // 2
    odd = r % 2
    pos = odd * (q - 1) + (1 - 2 * odd) * (r // 2)

    def owner_at(p):
        p = lax.rem(p + 2 * q, q)
        far = p // half_ring
        return far * (2 * (q - 1 - p) + 1) + (1 - far) * 2 * p

    targets = (zh * q + owner_at(pos + 1), zh * q + owner_at(pos - 1))

    barrier = pltpu.get_barrier_semaphore()
    me = s * tp + t
    for i in range(1, n * tp):
        other = lax.rem(me + i, n * tp)
        pl.semaphore_signal(
            barrier,
            inc=1,
            device_id={"sp": other // tp, "tp": lax.rem(other, tp)},
            device_id_type=MESH,
        )
    pl.semaphore_wait(barrier, n * tp - 1)

    copies = []
    guarded = []

    def remote(source, target, send, recv, sp_at, tp_at):
        return pltpu.make_async_remote_copy(
            src_ref=source,
            dst_ref=target,
            send_sem=send,
            recv_sem=recv,
            device_id={"sp": sp_at, "tp": tp_at},
            device_id_type=MESH,
        )

    def send(*args):
        copy = remote(*args)
        copy.start()
        copies.append(copy)
        return copy

    def send_or_keep(source, target, send_sem, recv_sem, sp_at, tp_at):
        away = (sp_at != s) | (tp_at != t)
        copy = remote(source, target, send_sem, recv_sem, sp_at, tp_at)

        @pl.when(away)
        def _():
            copy.start()

        @pl.when(jnp.logical_not(away))
        def _():
            pltpu.make_async_copy(source, target, recv_sem).start()

        guarded.append((away, copy))
        return copy

    def arrived(target, sem):
        pltpu.make_async_copy(target, target, sem).wait()

    pieces = (
        (0, w_key, own_key, key_in),
        (1, w_value, own_value, value_in),
        (2, w_query, own_query, query_in),
        (3, w_out, own_out, out_in),
    )
    stays = zh == c
    def first_send(p):
        _, own, stage, _ = pieces[p]
        width = own.shape[1] // 2
        for g in range(2):
            mine = own.at[:, pl.ds(g * width, width)]
            keep = stays & (c == g)
            block = (zh + c) % 2
            copy = remote(
                mine,
                stage.at[block],
                first_sems.at[g, p],
                first_recv.at[block, p],
                c * q + r,
                2 * y + g,
            )

            @pl.when(jnp.logical_not(keep))
            def _():
                copy.start()

            @pl.when(keep)
            def _():
                pltpu.make_async_copy(mine, stage.at[0], first_recv.at[0, p]).start()

            guarded.append((jnp.logical_not(keep), copy))

    for p in range(3):
        first_send(p)

    def ring_copy(p, block, d, k):
        _, _, stage, landing = pieces[p]
        size = stage.shape[1] // 2
        source = (
            stage.at[block, pl.ds(d * size, size)] if k == 0 else landing.at[block, d, k - 1]
        )
        return send(
            source,
            landing.at[block, d, k],
            ring_send.at[p, block, d, k],
            ring_recv.at[p, block, d, k],
            targets[d],
            t,
        )

    live = {}

    def ring_start(p, block):
        arrived(pieces[p][2].at[block], first_recv.at[block, p])
        for d in range(2):
            live[p, block, d] = ring_copy(p, block, d, 0)

    def ring_step(p, block, k):
        for d in range(2):
            live[p, block, d].wait_recv()
            if k + 1 < steps:
                live[p, block, d] = ring_copy(p, block, d, k + 1)

    cols = (slice(0, dk), slice(dk, dk + dv), slice(dk + dv, 2 * dk + dv))

    def origin(block, owner):
        return (zh if block == 0 else 1 - zh) * q + owner

    def own_product(block, fresh):
        at = pl.ds(pl.multiple_of(origin(block, r) * depth, depth), depth)
        part = normed[:, at]
        for p in range(3):
            product = jnp.dot(part, pieces[p][2][block], preferred_element_type=f32)
            acc[:, cols[p]] = product if fresh else acc[:, cols[p]] + product

    def step_product(block, k):
        for d in range(2):
            owner = owner_at(pos - 1 - k) if d == 0 else owner_at(pos + 1 + k)
            at = pl.ds(
                pl.multiple_of(origin(block, owner) * depth + d * half, half), half
            )
            part = normed[:, at]
            for p in range(3):
                acc[:, cols[p]] += jnp.dot(
                    part, pieces[p][3][block, d, k], preferred_element_type=f32
                )

    for p in range(3):
        ring_start(p, 0)
    half_tp = tp // 2
    x = s % 2
    row_at = pl.ds(pl.multiple_of(x * span_rows + t * rows, rows), rows)
    for g in range(2):
        for yy in range(half_tp):
            to_s, to_t = g * q + s // 2, 2 * yy + c
            send_or_keep(
                tokens,
                tok_all.at[row_at],
                tok_send.at[g, yy],
                tok_recv.at[x, y],
                to_s,
                to_t,
            )
            send_or_keep(
                drift,
                drift_in.at[x, y],
                drift_send.at[g, yy],
                drift_recv.at[x, y],
                to_s,
                to_t,
            )

    first_send(3)
    for k in range(steps):
        for p in range(3):
            ring_step(p, 0, k)
    for p in range(3):
        ring_start(p, 1)
    for k in range(steps - 1):
        for p in range(3):
            ring_step(p, 1, k)
    for xx in range(2):
        for yy in range(half_tp):
            at = pl.ds(
                pl.multiple_of(xx * span_rows + (2 * yy + c) * rows, rows), rows
            )
            arrived(tok_all.at[at], tok_recv.at[xx, yy])
            arrived(drift_in.at[xx, yy], drift_recv.at[xx, yy])
            send(
                tok_all.at[at],
                tok_all.at[at],
                near_send.at[xx, yy],
                near_recv.at[xx, yy],
                s,
                near,
            )
    for xx in range(2):
        for yy in range(half_tp):
            at = pl.ds(
                pl.multiple_of(xx * span_rows + (2 * yy + 1 - c) * rows, rows), rows
            )
            arrived(tok_all.at[at], near_recv.at[xx, yy])
    wide = tok_all[...].astype(f32)
    scale = lax.rsqrt(jnp.mean(wide * wide, axis=1, keepdims=True) + norm_floor)
    normed[...] = (wide * scale * pre_gain[...].astype(f32)[None, :]).astype(bf16)

    ring_start(3, 0)
    own_product(0, True)
    for k in range(steps):
        step_product(0, k)
    own_product(1, False)
    for k in range(steps - 1):
        step_product(1, k)
    all_normed = normed[...]
    gate_in = dot_nt(all_normed, w_igate[...])
    gate_forget = dot_nt(all_normed, w_fgate[...])
    row_id = lax.broadcasted_iota(jnp.int32, (length, length), 0)
    col_id = lax.broadcasted_iota(jnp.int32, (length, length), 1)
    causal = row_id >= col_id
    pick = lax.broadcasted_iota(jnp.int32, gate_in.shape, 1) == head
    late = lax.broadcasted_iota(jnp.int32, (length, 1), 0) >= span_rows
    mine = pl.ds(head, 1)
    offset = jnp.where(late, drift_in[1, 0, mine, :][:, :1], drift_in[0, 0, mine, :][:, :1])
    forget_pre = (
        jnp.sum(jnp.where(pick, gate_forget, 0.0), axis=1, keepdims=True)
        + forget_bias[head]
        + offset
    )
    lf_col = jnp.minimum(forget_pre, 0.0) - jnp.log1p(jnp.exp(-jnp.abs(forget_pre)))
    in_col = jnp.sum(jnp.where(pick, gate_in, 0.0), axis=1, keepdims=True)
    lf_row = jnp.sum(jnp.where(row_id == col_id, lf_col, 0.0), axis=0, keepdims=True)
    in_row = jnp.sum(jnp.where(row_id == col_id, in_col, 0.0), axis=0, keepdims=True)
    b_col = jnp.sum(jnp.where(causal, lf_row, 0.0), axis=1, keepdims=True)
    b_row = jnp.sum(jnp.where(row_id <= col_id, lf_col, 0.0), axis=0, keepdims=True)
    span = jnp.sum(lf_col, axis=0, keepdims=True)
    write = span - b_col + in_col
    top = jnp.max(write, axis=0, keepdims=True)
    write_scale = jnp.exp(write - top)
    log_pair = jnp.where(causal, b_col - b_row + in_row, lowest_log)
    peak = jnp.max(log_pair, axis=1, keepdims=True)
    decay = jnp.where(causal, jnp.exp(log_pair - peak), 0.0)

    ring_step(3, 0, 0)
    for p in range(3):
        ring_step(p, 1, steps - 1)
    step_product(1, steps - 1)
    ring_start(3, 1)

    keys = (acc[:, cols[0]] * (dk**-0.5)).astype(bf16)
    values = acc[:, cols[1]].astype(bf16)
    queries = acc[:, cols[2]].astype(bf16)
    key_scaled = keys.astype(f32) * write_scale
    state_own[...] = jnp.dot(
        key_scaled.T.astype(bf16), values, preferred_element_type=f32
    ).astype(bf16)
    aux_own[0:1, :] = jnp.broadcast_to(span, (1, dk))
    aux_own[1:2, :] = jnp.broadcast_to(top, (1, dk))
    aux_own[2:3, :] = jnp.sum(key_scaled, axis=0, keepdims=True)
    aux_own[3:, :] = jnp.zeros((aux_own.shape[0] - 3, dk), f32)
    state_copies = []
    for i in range(1, q):
        peer = zh * q + lax.rem(r + i, q)
        state_copies.append(
            (
                send(
                    state_own,
                    state_in.at[i - 1],
                    state_send.at[i - 1],
                    state_recv.at[i - 1],
                    peer,
                    t,
                ),
                send(
                    aux_own,
                    aux_in.at[i - 1],
                    aux_send.at[i - 1],
                    aux_recv.at[i - 1],
                    peer,
                    t,
                ),
            )
        )
    weights = dot_nt(queries, keys) * decay
    numer = jnp.dot(weights.astype(bf16), values, preferred_element_type=f32)
    denom = jnp.sum(weights, axis=1, keepdims=True)
    for k in range(1, steps):
        ring_step(3, 0, k)
        ring_step(3, 1, k - 1)

    for pair in state_copies:
        for copy in pair:
            copy.wait_recv()
    owners = [lax.rem(r - i + q, q) for i in range(1, q)]
    logs = []
    for k in range(steps):
        total = aux_in[k, 1:2, :]
        for i in range(steps):
            if i != k:
                between = when((owners[i] > owners[k]) & (owners[i] < r))
                total = total + between * aux_in[i, 0:1, :]
        before = when(owners[k] < r)
        logs.append((before, before * total + (1.0 - before) * lowest_log))
    entry = functools.reduce(jnp.maximum, [log for _, log in logs])
    mat = jnp.zeros((dk, dv), f32)
    vec = jnp.zeros((1, dk), f32)
    for k in range(steps):
        before, log = logs[k]
        weight = before * jnp.exp(log - entry)
        mat = mat + weight[:, :1] * state_in[k].astype(f32)
        vec = vec + weight * aux_in[k, 2:3, :]
    carried = b_col + entry[:, :1]
    new_top = jnp.maximum(peak, carried)
    w_intra = jnp.exp(peak - new_top)
    w_carry = jnp.exp(carried - new_top)
    numer = w_intra * numer + w_carry * jnp.dot(
        queries, mat.astype(bf16), preferred_element_type=f32
    )
    denom = w_intra * denom + w_carry * jnp.sum(
        queries.astype(f32) * vec, axis=1, keepdims=True
    )
    hidden = numer / jnp.maximum(jnp.abs(denom), jnp.exp(-new_top))
    gain = head_gain[pl.ds(pl.multiple_of(head * dv, dv), dv)].astype(f32)[None, :]
    heads[...] = (
        hidden
        * lax.rsqrt(jnp.mean(hidden * hidden, axis=1, keepdims=True) + norm_floor)
        * gain
    ).astype(bf16)

    ready = heads[...]
    e_depth = w_out.shape[0]
    e_half = e_depth // 2
    wide_half = q * e_depth
    theirs = pl.ds(pl.multiple_of((1 - c) * span_rows, span_rows), span_rows)
    kept = pl.ds(pl.multiple_of(c * span_rows, span_rows), span_rows)

    def share_own(block):
        at = pl.ds(pl.multiple_of(r * e_depth, e_depth), e_depth)
        shares[block, :, at] = dot_nt(ready, own_out[block]).astype(bf16)

    def share_step(block, k):
        for d in range(2):
            owner = owner_at(pos - 1 - k) if d == 0 else owner_at(pos + 1 + k)
            at = pl.ds(pl.multiple_of(owner * e_depth + d * e_half, e_half), e_half)
            shares[block, :, at] = dot_nt(ready, out_in[block, d, k]).astype(bf16)

    def pair_start(block):
        return send(
            shares.at[block, theirs],
            pair_in.at[block],
            pair_send.at[block],
            pair_recv.at[block],
            s,
            near,
        )

    def share_out(block, pair):
        pair.wait_recv()
        pair_sum[block] = (
            shares[block, kept, :].astype(f32) + pair_in[block].astype(f32)
        ).astype(bf16)
        side = zh if block == 0 else 1 - zh
        for to_t in range(tp):
            send_or_keep(
                pair_sum.at[block, pl.ds(to_t * rows, rows)],
                shares_in.at[zh, y, side],
                share_send.at[block, to_t],
                share_recv.at[zh, y, side],
                2 * r + c,
                to_t,
            )

    share_own(0)
    for k in range(steps):
        share_step(0, k)
    pair = pair_start(0)
    share_own(1)
    for k in range(steps - 1):
        share_step(1, k)
    share_out(0, pair)
    ring_step(3, 1, steps - 1)
    share_step(1, steps - 1)
    share_out(1, pair_start(1))
    for side in range(2):
        total = jnp.zeros((rows, wide_half), f32)
        for g in range(2):
            for yy in range(half_tp):
                arrived(shares_in.at[g, yy, side], share_recv.at[g, yy, side])
                total = total + shares_in[g, yy, side].astype(f32)
        out[:, side * wide_half : (side + 1) * wide_half] = total.astype(bf16)
    for copy in copies:
        copy.wait_send()
    for away, copy in guarded:

        @pl.when(away)
        def _():
            copy.wait_send()


def on_device_ring(
    n,
    tp,
    tokens,
    pre_gain,
    w_query,
    w_key,
    w_value,
    w_igate,
    w_fgate,
    forget_bias,
    gate_drift,
    head_gain,
    w_out,
):
    heads = w_igate.shape[1]
    if heads != 2 * tp or gate_drift.shape[0] > drift_span:
        return on_device(
            tokens,
            pre_gain,
            w_query,
            w_key,
            w_value,
            w_igate,
            w_fgate,
            forget_bias,
            gate_drift,
            head_gain,
            w_out,
        )
    rows, width = tokens.shape
    length = 2 * rows * tp
    q = n // 2
    steps = q - 1
    half_tp = tp // 2
    dk = w_query.shape[1] // 2
    dv = w_value.shape[1] // 2
    features = w_out.shape[0] * n
    vmem = pl.BlockSpec(memory_space=pltpu.VMEM)
    dma = pltpu.SemaphoreType.DMA
    weights = (w_key, w_value, w_query, w_out)
    smem = pl.BlockSpec(memory_space=pltpu.SMEM)
    return pl.pallas_call(
        functools.partial(square_kernel, n, tp),
        out_shape=jax.ShapeDtypeStruct((rows, features), bf16),
        in_specs=[vmem] * 7 + [smem] + [vmem] * 3,
        out_specs=vmem,
        scratch_shapes=[
            pltpu.VMEM((length, width), bf16),
            pltpu.VMEM((2, half_tp, heads, gate_drift.shape[0]), f32),
            pltpu.VMEM((length, width), bf16),
            *[pltpu.VMEM((2, w.shape[0], w.shape[1] // 2), bf16) for w in weights],
            *[
                pltpu.VMEM((2, 2, steps, w.shape[0] // 2, w.shape[1] // 2), bf16)
                for w in weights
            ],
            pltpu.VMEM((dk, dv), bf16),
            pltpu.VMEM((steps, dk, dv), bf16),
            pltpu.VMEM((8, dk), f32),
            pltpu.VMEM((steps, 8, dk), f32),
            pltpu.VMEM((length, 2 * dk + dv), f32),
            pltpu.VMEM((length, dv), bf16),
            pltpu.VMEM((2, length, features // 2), bf16),
            pltpu.VMEM((2, length // 2, features // 2), bf16),
            pltpu.VMEM((2, length // 2, features // 2), bf16),
            pltpu.VMEM((2, half_tp, 2, rows, features // 2), bf16),
            dma((2, half_tp)),
            dma((2, half_tp)),
            dma((2, half_tp)),
            dma((2, half_tp)),
            dma((2, half_tp)),
            dma((2, half_tp)),
            dma((2, 4)),
            dma((2, 4)),
            dma((4, 2, 2, steps)),
            dma((4, 2, 2, steps)),
            dma((steps,)),
            dma((steps,)),
            dma((steps,)),
            dma((steps,)),
            dma((2,)),
            dma((2,)),
            dma((2, tp)),
            dma((2, half_tp, 2)),
        ],
        compiler_params=pltpu.CompilerParams(collective_id=0, has_side_effects=True),
    )(
        tokens,
        pre_gain,
        w_query,
        w_key,
        w_value,
        w_igate.T,
        w_fgate.T,
        forget_bias,
        gate_drift.T,
        head_gain,
        w_out,
    )


def solution(mesh):
    in_specs = (
        P(("sp", "tp"), None),
        P(),
        P("sp", "tp"),
        P("sp", "tp"),
        P("sp", "tp"),
        P(),
        P(),
        P(),
        P("sp", None),
        P(),
        P("sp", "tp"),
    )
    out_specs = P(("sp", "tp"), None)
    body = on_device
    if mesh.shape["sp"] <= ring_limit and mesh.shape["sp"] % 4 == 0 and mesh.shape["tp"] % 2 == 0:
        body = functools.partial(on_device_ring, mesh.shape["sp"], mesh.shape["tp"])
    return jax.shard_map(
        body, mesh=mesh, in_specs=in_specs, out_specs=out_specs, check_vma=False
    )
```

```python
import functools

import jax
import jax.numpy as jnp
from jax import lax
from jax.experimental import pallas as pl
from jax.experimental.pallas import tpu as pltpu
from jax.sharding import PartitionSpec as P

BLOCK = 64


norm_floor = 0.1
lowest_log = -1e30
highest = lax.Precision.HIGHEST


def prefix(value, axis, combine, identity):
    peers, position = (lax.axis_size(axis), lax.axis_index(axis))
    everything = jax.tree.map(
        lambda part, kind: lax.all_gather(part.astype(kind), axis),
        value,
        jax.tree.map(lambda a: jnp.bfloat16 if a.dtype == jnp.float32 else a.dtype, value),
    )
    start = jax.tree.map(
        lambda part, zero: jnp.broadcast_to(jnp.asarray(zero, part.dtype), part.shape),
        value,
        identity,
    )

    def step(k, before):
        reached = k < position
        new = combine(
            before, jax.tree.map(lambda part, own: part[k].astype(own.dtype), everything, value)
        )
        return jax.tree.map(lambda a, b: jnp.where(reached, a, b), new, before)

    return lax.fori_loop(0, peers, step, start)


def advance(memory, summary):
    old_mat, old_vec, old_top = memory
    span_log, span_top, span_mat, span_vec = summary
    new_top = jnp.maximum(span_log + old_top, span_top)
    kept_part = jnp.exp(span_log + old_top - new_top)
    fresh_part = jnp.exp(span_top - new_top)
    return (
        kept_part[:, None, None] * old_mat + fresh_part[:, None, None] * span_mat,
        kept_part[:, None] * old_vec + fresh_part[:, None] * span_vec,
        new_top,
    )


def prefix_states(initial, summary):

    def stepper(memory, one_block):
        return (advance(memory, one_block), memory)

    return lax.scan(stepper, initial, summary)


def join_devices(earlier, later_part):
    early_log, early_mat, early_vec, early_top = earlier
    late_log, late_mat, late_vec, late_top = later_part
    new_top = jnp.maximum(late_log + early_top, late_top)
    kept_part = jnp.exp(late_log + early_top - new_top)
    fresh_part = jnp.exp(late_top - new_top)
    return (
        early_log + late_log,
        kept_part[:, None, None] * early_mat + fresh_part[:, None, None] * late_mat,
        kept_part[:, None] * early_vec + fresh_part[:, None] * late_vec,
        new_top,
    )


def blend_parts(first_part, second_part):
    numer_first, denom_first, peak_first = first_part
    numer_second, denom_second, peak_second = second_part
    new_top = jnp.maximum(peak_first, peak_second)
    weight_first = jnp.exp(peak_first - new_top)
    weight_second = jnp.exp(peak_second - new_top)
    return (
        weight_first[..., None] * numer_first + weight_second[..., None] * numer_second,
        weight_first * denom_first + weight_second * denom_second,
        new_top,
    )


def on_device(
    tokens,
    pre_gain,
    w_query,
    w_key,
    w_value,
    w_igate,
    w_fgate,
    forget_bias,
    gate_drift,
    head_gain,
    w_out,
):
    tp_size = lax.axis_size("tp")
    head_count = w_igate.shape[1]
    local_heads = head_count // tp_size
    first_head = lax.axis_index("tp") * local_heads
    key_width = w_query.shape[1] // local_heads
    value_width = w_value.shape[1] // local_heads
    token_wide = tokens.astype(jnp.float32)
    scaled = token_wide * lax.rsqrt(
        jnp.mean(token_wide * token_wide, axis=1, keepdims=True) + norm_floor
    )
    normed = (scaled * pre_gain.astype(jnp.float32)).astype(jnp.bfloat16)
    gate_cols = jnp.concatenate(
        [
            lax.dynamic_slice_in_dim(w_igate, first_head, local_heads, 1),
            lax.dynamic_slice_in_dim(w_fgate, first_head, local_heads, 1),
        ],
        axis=1,
    )
    key_scale = key_width ** (-0.5)
    wq_full, wk_full, wv_full = (
        lax.all_gather(w_query, "sp", axis=0, tiled=True),
        lax.all_gather(w_key, "sp", axis=0, tiled=True),
        lax.all_gather(w_value, "sp", axis=0, tiled=True),
    )
    row_piece = lax.all_gather(normed, "tp", axis=0, tiled=True)
    queries_part = jnp.dot(row_piece, wq_full, preferred_element_type=jnp.float32).astype(
        jnp.bfloat16
    )
    keys_part = (
        jnp.dot(row_piece, wk_full, preferred_element_type=jnp.float32) * key_scale
    ).astype(jnp.bfloat16)
    values_part = jnp.dot(row_piece, wv_full, preferred_element_type=jnp.float32).astype(
        jnp.bfloat16
    )
    gate_part = jnp.dot(row_piece, gate_cols, preferred_element_type=jnp.float32)
    group_len = queries_part.shape[0]
    blocks = group_len // BLOCK
    log_input = gate_part[:, :local_heads]
    forget_pre = gate_part[:, local_heads:] + lax.dynamic_slice_in_dim(
        forget_bias, first_head, local_heads, 0
    )
    log_forget = jax.nn.log_sigmoid(
        forget_pre + lax.dynamic_slice_in_dim(gate_drift, first_head, local_heads, 1)
    )
    query_blk = queries_part.reshape(blocks, BLOCK, local_heads, key_width)
    key_blk = keys_part.reshape(blocks, BLOCK, local_heads, key_width)
    value_blk = values_part.reshape(blocks, BLOCK, local_heads, value_width)
    input_blk = log_input.reshape(blocks, BLOCK, local_heads).transpose(0, 2, 1)
    forget_blk = log_forget.reshape(blocks, BLOCK, local_heads).transpose(0, 2, 1)
    within = jnp.cumsum(forget_blk, axis=2)
    causal = jnp.arange(BLOCK)[:, None] >= jnp.arange(BLOCK)[None, :]
    log_pair = jnp.where(
        causal, within[..., :, None] - within[..., None, :] + input_blk[..., None, :], -jnp.inf
    )
    peak_intra = jnp.max(log_pair, axis=3)
    scores = jnp.einsum("nshd,nrhd->nhsr", query_blk, key_blk, preferred_element_type=jnp.float32)
    weights = scores * jnp.exp(log_pair - peak_intra[..., None])
    numer_intra = jnp.einsum(
        "nhsr,nrhv->nhsv",
        weights.astype(jnp.bfloat16),
        value_blk,
        preferred_element_type=jnp.float32,
    )
    denom_intra = jnp.sum(weights, axis=3)
    span_log = within[..., -1]
    log_write = span_log[..., None] - within + input_blk
    span_top = jnp.max(log_write, axis=2)
    write_scale = jnp.exp(log_write - span_top[..., None])
    key_scaled = key_blk.astype(jnp.float32) * write_scale.transpose(0, 2, 1)[..., None]
    value_wide = value_blk.astype(jnp.float32)
    span_mat = jnp.einsum("nrhv,nrhd->nhvd", value_wide, key_scaled, precision=highest)
    span_vec = jnp.sum(key_scaled, axis=1)
    summary = (span_log, span_top, span_mat, span_vec)
    empty_state = (
        jnp.zeros((local_heads, value_width, key_width), jnp.float32),
        jnp.zeros((local_heads, key_width), jnp.float32),
        jnp.full((local_heads,), lowest_log, jnp.float32),
    )
    local_end, local_starts = prefix_states(empty_state, summary)
    device_summary = (jnp.sum(span_log, axis=0),) + local_end
    identity_all = (jnp.zeros((local_heads,), jnp.float32),) + empty_state
    incoming = prefix(device_summary, "sp", join_devices, identity_all)
    query_wide = query_blk.astype(jnp.float32)
    intra_part = (numer_intra, denom_intra, peak_intra)
    start_mat, start_vec, start_top = local_starts
    local_part = (
        jnp.einsum("nhvd,nshd->nhsv", start_mat, query_wide, precision=highest),
        jnp.einsum("nhd,nshd->nhs", start_vec, query_wide, precision=highest),
        within + start_top[..., None],
    )
    numerator, denominator, peak_log = blend_parts(local_part, intra_part)
    entry_log, entry_mat, entry_vec, entry_top = incoming
    before_log = jnp.concatenate(
        [jnp.zeros((1, local_heads), jnp.float32), jnp.cumsum(span_log, axis=0)[:-1]], axis=0
    )
    from_left = (
        jnp.einsum("hvd,nshd->nhsv", entry_mat, query_wide, precision=highest),
        jnp.einsum("hd,nshd->nhs", entry_vec, query_wide, precision=highest),
        within + (before_log + entry_top[None, :])[..., None],
    )
    numerator, denominator, peak_log = blend_parts((numerator, denominator, peak_log), from_left)
    hidden = numerator / jnp.maximum(jnp.abs(denominator), jnp.exp(-peak_log))[..., None]
    hidden = hidden.transpose(0, 2, 1, 3).reshape(group_len, local_heads, value_width)
    head_gains = lax.dynamic_slice_in_dim(
        head_gain, first_head * value_width, local_heads * value_width, 0
    )
    head_gains = head_gains.astype(jnp.float32).reshape(local_heads, value_width)
    normed_heads = (
        hidden
        * lax.rsqrt(jnp.mean(hidden * hidden, axis=2, keepdims=True) + norm_floor)
        * head_gains
    )
    normed_heads = normed_heads.astype(jnp.bfloat16).reshape(group_len, local_heads * value_width)
    out_slab = lax.all_gather(w_out, "sp", axis=0, tiled=True)
    return lax.psum_scatter(
        lax.dot_general(
            normed_heads, out_slab, (((1,), (1,)), ((), ())), preferred_element_type=jnp.float32
        ).astype(jnp.bfloat16),
        "tp",
        scatter_dimension=0,
        tiled=True,
    )


ring_limit = 16
drift_span = 128
MESH = pl.DeviceIdType.MESH
f32 = jnp.float32
bf16 = jnp.bfloat16


def dot_nt(a, b):
    return lax.dot_general(a, b, (((1,), (1,)), ((), ())), preferred_element_type=f32)


def when(flag):
    return flag.astype(jnp.int32).astype(f32)


def square_kernel(
    n,
    tp,
    tokens,
    pre_gain,
    w_query,
    w_key,
    w_value,
    w_igate,
    w_fgate,
    forget_bias,
    drift,
    head_gain,
    w_out,
    out,
    tok_all,
    drift_in,
    normed,
    own_key,
    own_value,
    own_query,
    own_out,
    key_in,
    value_in,
    query_in,
    out_in,
    state_own,
    state_in,
    aux_own,
    aux_in,
    acc,
    heads,
    shares,
    pair_in,
    pair_sum,
    shares_in,
    tok_send,
    tok_recv,
    drift_send,
    drift_recv,
    near_send,
    near_recv,
    far_send,
    far_recv,
    first_sems,
    first_recv,
    ring_send,
    ring_recv,
    state_send,
    state_recv,
    aux_send,
    aux_recv,
    pair_send,
    pair_recv,
    share_send,
    share_recv,
):
    s = lax.axis_index("sp")
    t = lax.axis_index("tp")
    q = n // 2
    steps = q - 1
    zh = s // q
    r = s % q
    y = t // 2
    c = t % 2
    near = 2 * y + 1 - c
    head = 2 * (2 * y + zh) + c
    rows = tokens.shape[0]
    span_rows = rows * tp
    length = 2 * span_rows
    dk = w_query.shape[1] // 2
    dv = w_value.shape[1] // 2
    depth = w_query.shape[0]
    half = depth // 2
    half_ring = q // 2
    odd = r % 2
    pos = odd * (q - 1) + (1 - 2 * odd) * (r // 2)

    def owner_at(p):
        p = lax.rem(p + 2 * q, q)
        far = p // half_ring
        return far * (2 * (q - 1 - p) + 1) + (1 - far) * 2 * p

    targets = (zh * q + owner_at(pos + 1), zh * q + owner_at(pos - 1))

    barrier = pltpu.get_barrier_semaphore()
    me = s * tp + t
    for i in range(1, n * tp):
        other = lax.rem(me + i, n * tp)
        pl.semaphore_signal(
            barrier,
            inc=1,
            device_id={"sp": other // tp, "tp": lax.rem(other, tp)},
            device_id_type=MESH,
        )
    pl.semaphore_wait(barrier, n * tp - 1)

    copies = []
    guarded = []

    def remote(source, target, send, recv, sp_at, tp_at):
        return pltpu.make_async_remote_copy(
            src_ref=source,
            dst_ref=target,
            send_sem=send,
            recv_sem=recv,
            device_id={"sp": sp_at, "tp": tp_at},
            device_id_type=MESH,
        )

    def send(*args):
        copy = remote(*args)
        copy.start()
        copies.append(copy)
        return copy

    def send_or_keep(source, target, send_sem, recv_sem, sp_at, tp_at):
        away = (sp_at != s) | (tp_at != t)
        copy = remote(source, target, send_sem, recv_sem, sp_at, tp_at)

        @pl.when(away)
        def _():
            copy.start()

        @pl.when(jnp.logical_not(away))
        def _():
            pltpu.make_async_copy(source, target, recv_sem).start()

        guarded.append((away, copy))
        return copy

    def arrived(target, sem):
        pltpu.make_async_copy(target, target, sem).wait()

    pieces = (
        (0, w_key, own_key, key_in),
        (1, w_value, own_value, value_in),
        (2, w_query, own_query, query_in),
        (3, w_out, own_out, out_in),
    )
    stays = zh == c
    def first_send(p):
        _, own, stage, _ = pieces[p]
        width = own.shape[1] // 2
        for g in range(2):
            mine = own.at[:, pl.ds(g * width, width)]
            keep = stays & (c == g)
            block = (zh + c) % 2
            copy = remote(
                mine,
                stage.at[block],
                first_sems.at[g, p],
                first_recv.at[block, p],
                c * q + r,
                2 * y + g,
            )

            @pl.when(jnp.logical_not(keep))
            def _():
                copy.start()

            @pl.when(keep)
            def _():
                pltpu.make_async_copy(mine, stage.at[0], first_recv.at[0, p]).start()

            guarded.append((jnp.logical_not(keep), copy))

    for p in range(3):
        first_send(p)

    def ring_copy(p, block, d, k):
        _, _, stage, landing = pieces[p]
        size = stage.shape[1] // 2
        source = (
            stage.at[block, pl.ds(d * size, size)] if k == 0 else landing.at[block, d, k - 1]
        )
        return send(
            source,
            landing.at[block, d, k],
            ring_send.at[p, block, d, k],
            ring_recv.at[p, block, d, k],
            targets[d],
            t,
        )

    live = {}

    def ring_start(p, block):
        arrived(pieces[p][2].at[block], first_recv.at[block, p])
        for d in range(2):
            live[p, block, d] = ring_copy(p, block, d, 0)

    def ring_step(p, block, k):
        for d in range(2):
            live[p, block, d].wait_recv()
            if k + 1 < steps:
                live[p, block, d] = ring_copy(p, block, d, k + 1)

    cols = (slice(0, dk), slice(dk, dk + dv), slice(dk + dv, 2 * dk + dv))

    def origin(block, owner):
        return (zh if block == 0 else 1 - zh) * q + owner

    def own_product(block, fresh):
        at = pl.ds(pl.multiple_of(origin(block, r) * depth, depth), depth)
        part = normed[:, at]
        for p in range(3):
            product = jnp.dot(part, pieces[p][2][block], preferred_element_type=f32)
            acc[:, cols[p]] = product if fresh else acc[:, cols[p]] + product

    def step_product(block, k):
        for d in range(2):
            owner = owner_at(pos - 1 - k) if d == 0 else owner_at(pos + 1 + k)
            at = pl.ds(
                pl.multiple_of(origin(block, owner) * depth + d * half, half), half
            )
            part = normed[:, at]
            for p in range(3):
                acc[:, cols[p]] += jnp.dot(
                    part, pieces[p][3][block, d, k], preferred_element_type=f32
                )

    for p in range(3):
        ring_start(p, 0)
    half_tp = tp // 2
    x = s % 2
    row_at = pl.ds(pl.multiple_of(x * span_rows + t * rows, rows), rows)

    def tokens_at(xx, to_t):
        start = pl.multiple_of(xx * span_rows + to_t * rows, rows)
        return tok_all.at[pl.ds(start, rows)]

    for p in range(3):
        ring_step(p, 0, 0)
    for g in range(2):
        to_s = g * q + s // 2
        send_or_keep(
            tokens, tok_all.at[row_at], tok_send.at[g], tok_recv.at[x], to_s, t
        )
        send_or_keep(
            drift, drift_in.at[x], drift_send.at[g], drift_recv.at[x], to_s, t
        )
    for k in range(1, steps):
        for p in range(3):
            ring_step(p, 0, k)
    first_send(3)
    for p in range(3):
        ring_start(p, 1)
    for xx in range(2):
        block = tokens_at(xx, t)
        arrived(block, tok_recv.at[xx])
        arrived(drift_in.at[xx], drift_recv.at[xx])
        for i in range(1, half_tp):
            far_t = 2 * lax.rem(y + i, half_tp) + c
            send(block, block, far_send.at[xx, i - 1], far_recv.at[xx, i - 1], s, far_t)
        send(block, block, near_send.at[xx, 0], near_recv.at[xx, 0], s, near)
    for p in range(3):
        ring_step(p, 1, 0)
    for xx in range(2):
        for i in range(1, half_tp):
            block = tokens_at(xx, 2 * lax.rem(y - i + half_tp, half_tp) + c)
            arrived(block, far_recv.at[xx, i - 1])
            send(block, block, near_send.at[xx, i], near_recv.at[xx, i], s, near)
    for k in range(1, steps - 1):
        for p in range(3):
            ring_step(p, 1, k)
    ring_start(3, 0)
    for xx in range(2):
        for i in range(half_tp):
            block = tokens_at(xx, 2 * lax.rem(y - i + half_tp, half_tp) + 1 - c)
            arrived(block, near_recv.at[xx, i])
    wide = tok_all[...].astype(f32)
    scale = lax.rsqrt(jnp.mean(wide * wide, axis=1, keepdims=True) + norm_floor)
    normed[...] = (wide * scale * pre_gain[...].astype(f32)[None, :]).astype(bf16)

    own_product(0, True)
    for k in range(steps):
        step_product(0, k)
    own_product(1, False)
    for k in range(steps - 1):
        step_product(1, k)
    all_normed = normed[...]
    gate_in = dot_nt(all_normed, w_igate[...])
    gate_forget = dot_nt(all_normed, w_fgate[...])
    row_id = lax.broadcasted_iota(jnp.int32, (length, length), 0)
    col_id = lax.broadcasted_iota(jnp.int32, (length, length), 1)
    causal = row_id >= col_id
    pick = lax.broadcasted_iota(jnp.int32, gate_in.shape, 1) == head
    late = lax.broadcasted_iota(jnp.int32, (length, 1), 0) >= span_rows
    mine = pl.ds(head, 1)
    offset = jnp.where(late, drift_in[1, mine, :][:, :1], drift_in[0, mine, :][:, :1])
    forget_pre = (
        jnp.sum(jnp.where(pick, gate_forget, 0.0), axis=1, keepdims=True)
        + forget_bias[head]
        + offset
    )
    lf_col = jnp.minimum(forget_pre, 0.0) - jnp.log1p(jnp.exp(-jnp.abs(forget_pre)))
    in_col = jnp.sum(jnp.where(pick, gate_in, 0.0), axis=1, keepdims=True)
    lf_row = jnp.sum(jnp.where(row_id == col_id, lf_col, 0.0), axis=0, keepdims=True)
    in_row = jnp.sum(jnp.where(row_id == col_id, in_col, 0.0), axis=0, keepdims=True)
    b_col = jnp.sum(jnp.where(causal, lf_row, 0.0), axis=1, keepdims=True)
    b_row = jnp.sum(jnp.where(row_id <= col_id, lf_col, 0.0), axis=0, keepdims=True)
    span = jnp.sum(lf_col, axis=0, keepdims=True)
    write = span - b_col + in_col
    top = jnp.max(write, axis=0, keepdims=True)
    write_scale = jnp.exp(write - top)
    log_pair = jnp.where(causal, b_col - b_row + in_row, lowest_log)
    peak = jnp.max(log_pair, axis=1, keepdims=True)
    decay = jnp.where(causal, jnp.exp(log_pair - peak), 0.0)

    ring_step(3, 0, 0)
    for p in range(3):
        ring_step(p, 1, steps - 1)
    step_product(1, steps - 1)
    ring_start(3, 1)

    keys = (acc[:, cols[0]] * (dk**-0.5)).astype(bf16)
    values = acc[:, cols[1]].astype(bf16)
    queries = acc[:, cols[2]].astype(bf16)
    key_scaled = keys.astype(f32) * write_scale
    state_own[...] = jnp.dot(
        key_scaled.T.astype(bf16), values, preferred_element_type=f32
    ).astype(bf16)
    aux_own[0:1, :] = jnp.broadcast_to(span, (1, dk))
    aux_own[1:2, :] = jnp.broadcast_to(top, (1, dk))
    aux_own[2:3, :] = jnp.sum(key_scaled, axis=0, keepdims=True)
    aux_own[3:, :] = jnp.zeros((aux_own.shape[0] - 3, dk), f32)
    state_copies = []
    for i in range(1, q):
        peer = zh * q + lax.rem(r + i, q)
        state_copies.append(
            (
                send(
                    state_own,
                    state_in.at[i - 1],
                    state_send.at[i - 1],
                    state_recv.at[i - 1],
                    peer,
                    t,
                ),
                send(
                    aux_own,
                    aux_in.at[i - 1],
                    aux_send.at[i - 1],
                    aux_recv.at[i - 1],
                    peer,
                    t,
                ),
            )
        )
    weights = dot_nt(queries, keys) * decay
    numer = jnp.dot(weights.astype(bf16), values, preferred_element_type=f32)
    denom = jnp.sum(weights, axis=1, keepdims=True)
    ring_step(3, 0, 1)
    ring_step(3, 1, 0)
    for pair in state_copies:
        for copy in pair:
            copy.wait_recv()
    owners = [lax.rem(r - i + q, q) for i in range(1, q)]
    logs = []
    for k in range(steps):
        total = aux_in[k, 1:2, :]
        for i in range(steps):
            if i != k:
                between = when((owners[i] > owners[k]) & (owners[i] < r))
                total = total + between * aux_in[i, 0:1, :]
        before = when(owners[k] < r)
        logs.append((before, before * total + (1.0 - before) * lowest_log))
    entry = functools.reduce(jnp.maximum, [log for _, log in logs])
    mat = jnp.zeros((dk, dv), f32)
    vec = jnp.zeros((1, dk), f32)
    for k in range(steps):
        before, log = logs[k]
        weight = before * jnp.exp(log - entry)
        mat = mat + weight[:, :1] * state_in[k].astype(f32)
        vec = vec + weight * aux_in[k, 2:3, :]
    carried = b_col + entry[:, :1]
    new_top = jnp.maximum(peak, carried)
    w_intra = jnp.exp(peak - new_top)
    w_carry = jnp.exp(carried - new_top)
    numer = w_intra * numer + w_carry * jnp.dot(
        queries, mat.astype(bf16), preferred_element_type=f32
    )
    denom = w_intra * denom + w_carry * jnp.sum(
        queries.astype(f32) * vec, axis=1, keepdims=True
    )
    hidden = numer / jnp.maximum(jnp.abs(denom), jnp.exp(-new_top))
    gain = head_gain[pl.ds(pl.multiple_of(head * dv, dv), dv)].astype(f32)[None, :]
    heads[...] = (
        hidden
        * lax.rsqrt(jnp.mean(hidden * hidden, axis=1, keepdims=True) + norm_floor)
        * gain
    ).astype(bf16)

    ready = heads[...]
    e_depth = w_out.shape[0]
    e_half = e_depth // 2
    wide_half = q * e_depth
    theirs = pl.ds(pl.multiple_of((1 - c) * span_rows, span_rows), span_rows)
    kept = pl.ds(pl.multiple_of(c * span_rows, span_rows), span_rows)

    def share_own(block):
        at = pl.ds(pl.multiple_of(r * e_depth, e_depth), e_depth)
        shares[block, :, at] = dot_nt(ready, own_out[block]).astype(bf16)

    def share_step(block, k):
        for d in range(2):
            owner = owner_at(pos - 1 - k) if d == 0 else owner_at(pos + 1 + k)
            at = pl.ds(pl.multiple_of(owner * e_depth + d * e_half, e_half), e_half)
            shares[block, :, at] = dot_nt(ready, out_in[block, d, k]).astype(bf16)

    def pair_start(block):
        return send(
            shares.at[block, theirs],
            pair_in.at[block],
            pair_send.at[block],
            pair_recv.at[block],
            s,
            near,
        )

    def share_out(block, pair):
        pair.wait_recv()
        pair_sum[block] = (
            shares[block, kept, :].astype(f32) + pair_in[block].astype(f32)
        ).astype(bf16)
        side = zh if block == 0 else 1 - zh
        for to_t in range(tp):
            send_or_keep(
                pair_sum.at[block, pl.ds(to_t * rows, rows)],
                shares_in.at[zh, y, side],
                share_send.at[block, to_t],
                share_recv.at[zh, y, side],
                2 * r + c,
                to_t,
            )

    share_own(0)
    for k in range(steps):
        if k > 1:
            ring_step(3, 0, k)
        share_step(0, k)
    pair = pair_start(0)
    share_own(1)
    for k in range(steps - 1):
        if k > 0:
            ring_step(3, 1, k)
        share_step(1, k)
    share_out(0, pair)
    ring_step(3, 1, steps - 1)
    share_step(1, steps - 1)
    share_out(1, pair_start(1))
    for side in range(2):
        total = jnp.zeros((rows, wide_half), f32)
        for g in range(2):
            for yy in range(half_tp):
                arrived(shares_in.at[g, yy, side], share_recv.at[g, yy, side])
                total = total + shares_in[g, yy, side].astype(f32)
        out[:, side * wide_half : (side + 1) * wide_half] = total.astype(bf16)
    for copy in copies:
        copy.wait_send()
    for away, copy in guarded:

        @pl.when(away)
        def _():
            copy.wait_send()


def on_device_ring(
    n,
    tp,
    tokens,
    pre_gain,
    w_query,
    w_key,
    w_value,
    w_igate,
    w_fgate,
    forget_bias,
    gate_drift,
    head_gain,
    w_out,
):
    heads = w_igate.shape[1]
    if heads != 2 * tp or gate_drift.shape[0] > drift_span:
        return on_device(
            tokens,
            pre_gain,
            w_query,
            w_key,
            w_value,
            w_igate,
            w_fgate,
            forget_bias,
            gate_drift,
            head_gain,
            w_out,
        )
    rows, width = tokens.shape
    length = 2 * rows * tp
    q = n // 2
    steps = q - 1
    half_tp = tp // 2
    dk = w_query.shape[1] // 2
    dv = w_value.shape[1] // 2
    features = w_out.shape[0] * n
    vmem = pl.BlockSpec(memory_space=pltpu.VMEM)
    dma = pltpu.SemaphoreType.DMA
    weights = (w_key, w_value, w_query, w_out)
    smem = pl.BlockSpec(memory_space=pltpu.SMEM)
    return pl.pallas_call(
        functools.partial(square_kernel, n, tp),
        out_shape=jax.ShapeDtypeStruct((rows, features), bf16),
        in_specs=[vmem] * 7 + [smem] + [vmem] * 3,
        out_specs=vmem,
        scratch_shapes=[
            pltpu.VMEM((length, width), bf16),
            pltpu.VMEM((2, heads, gate_drift.shape[0]), f32),
            pltpu.VMEM((length, width), bf16),
            *[pltpu.VMEM((2, w.shape[0], w.shape[1] // 2), bf16) for w in weights],
            *[
                pltpu.VMEM((2, 2, steps, w.shape[0] // 2, w.shape[1] // 2), bf16)
                for w in weights
            ],
            pltpu.VMEM((dk, dv), bf16),
            pltpu.VMEM((steps, dk, dv), bf16),
            pltpu.VMEM((8, dk), f32),
            pltpu.VMEM((steps, 8, dk), f32),
            pltpu.VMEM((length, 2 * dk + dv), f32),
            pltpu.VMEM((length, dv), bf16),
            pltpu.VMEM((2, length, features // 2), bf16),
            pltpu.VMEM((2, length // 2, features // 2), bf16),
            pltpu.VMEM((2, length // 2, features // 2), bf16),
            pltpu.VMEM((2, half_tp, 2, rows, features // 2), bf16),
            dma((2,)),
            dma((2,)),
            dma((2,)),
            dma((2,)),
            dma((2, half_tp)),
            dma((2, half_tp)),
            dma((2, half_tp)),
            dma((2, half_tp)),
            dma((2, 4)),
            dma((2, 4)),
            dma((4, 2, 2, steps)),
            dma((4, 2, 2, steps)),
            dma((steps,)),
            dma((steps,)),
            dma((steps,)),
            dma((steps,)),
            dma((2,)),
            dma((2,)),
            dma((2, tp)),
            dma((2, half_tp, 2)),
        ],
        compiler_params=pltpu.CompilerParams(collective_id=0, has_side_effects=True),
    )(
        tokens,
        pre_gain,
        w_query,
        w_key,
        w_value,
        w_igate.T,
        w_fgate.T,
        forget_bias,
        gate_drift.T,
        head_gain,
        w_out,
    )


def solution(mesh):
    in_specs = (
        P(("sp", "tp"), None),
        P(),
        P("sp", "tp"),
        P("sp", "tp"),
        P("sp", "tp"),
        P(),
        P(),
        P(),
        P("sp", None),
        P(),
        P("sp", "tp"),
    )
    out_specs = P(("sp", "tp"), None)
    body = on_device
    if mesh.shape["sp"] <= ring_limit and mesh.shape["sp"] % 4 == 0 and mesh.shape["tp"] % 2 == 0:
        body = functools.partial(on_device_ring, mesh.shape["sp"], mesh.shape["tp"])
    return jax.shard_map(
        body, mesh=mesh, in_specs=in_specs, out_specs=out_specs, check_vma=False
    )
```

```python
import functools

import jax
import jax.numpy as jnp
from jax import lax
from jax.experimental import pallas as pl
from jax.experimental.pallas import tpu as pltpu
from jax.sharding import PartitionSpec as P

BLOCK = 64


norm_floor = 0.1
lowest_log = -1e30
highest = lax.Precision.HIGHEST


def prefix(value, axis, combine, identity):
    peers, position = (lax.axis_size(axis), lax.axis_index(axis))
    everything = jax.tree.map(
        lambda part, kind: lax.all_gather(part.astype(kind), axis),
        value,
        jax.tree.map(lambda a: jnp.bfloat16 if a.dtype == jnp.float32 else a.dtype, value),
    )
    start = jax.tree.map(
        lambda part, zero: jnp.broadcast_to(jnp.asarray(zero, part.dtype), part.shape),
        value,
        identity,
    )

    def step(k, before):
        reached = k < position
        new = combine(
            before, jax.tree.map(lambda part, own: part[k].astype(own.dtype), everything, value)
        )
        return jax.tree.map(lambda a, b: jnp.where(reached, a, b), new, before)

    return lax.fori_loop(0, peers, step, start)


def advance(memory, summary):
    old_mat, old_vec, old_top = memory
    span_log, span_top, span_mat, span_vec = summary
    new_top = jnp.maximum(span_log + old_top, span_top)
    kept_part = jnp.exp(span_log + old_top - new_top)
    fresh_part = jnp.exp(span_top - new_top)
    return (
        kept_part[:, None, None] * old_mat + fresh_part[:, None, None] * span_mat,
        kept_part[:, None] * old_vec + fresh_part[:, None] * span_vec,
        new_top,
    )


def prefix_states(initial, summary):

    def stepper(memory, one_block):
        return (advance(memory, one_block), memory)

    return lax.scan(stepper, initial, summary)


def join_devices(earlier, later_part):
    early_log, early_mat, early_vec, early_top = earlier
    late_log, late_mat, late_vec, late_top = later_part
    new_top = jnp.maximum(late_log + early_top, late_top)
    kept_part = jnp.exp(late_log + early_top - new_top)
    fresh_part = jnp.exp(late_top - new_top)
    return (
        early_log + late_log,
        kept_part[:, None, None] * early_mat + fresh_part[:, None, None] * late_mat,
        kept_part[:, None] * early_vec + fresh_part[:, None] * late_vec,
        new_top,
    )


def blend_parts(first_part, second_part):
    numer_first, denom_first, peak_first = first_part
    numer_second, denom_second, peak_second = second_part
    new_top = jnp.maximum(peak_first, peak_second)
    weight_first = jnp.exp(peak_first - new_top)
    weight_second = jnp.exp(peak_second - new_top)
    return (
        weight_first[..., None] * numer_first + weight_second[..., None] * numer_second,
        weight_first * denom_first + weight_second * denom_second,
        new_top,
    )


def on_device(
    tokens,
    pre_gain,
    w_query,
    w_key,
    w_value,
    w_igate,
    w_fgate,
    forget_bias,
    gate_drift,
    head_gain,
    w_out,
):
    tp_size = lax.axis_size("tp")
    head_count = w_igate.shape[1]
    local_heads = head_count // tp_size
    first_head = lax.axis_index("tp") * local_heads
    key_width = w_query.shape[1] // local_heads
    value_width = w_value.shape[1] // local_heads
    token_wide = tokens.astype(jnp.float32)
    scaled = token_wide * lax.rsqrt(
        jnp.mean(token_wide * token_wide, axis=1, keepdims=True) + norm_floor
    )
    normed = (scaled * pre_gain.astype(jnp.float32)).astype(jnp.bfloat16)
    gate_cols = jnp.concatenate(
        [
            lax.dynamic_slice_in_dim(w_igate, first_head, local_heads, 1),
            lax.dynamic_slice_in_dim(w_fgate, first_head, local_heads, 1),
        ],
        axis=1,
    )
    key_scale = key_width ** (-0.5)
    wq_full, wk_full, wv_full = (
        lax.all_gather(w_query, "sp", axis=0, tiled=True),
        lax.all_gather(w_key, "sp", axis=0, tiled=True),
        lax.all_gather(w_value, "sp", axis=0, tiled=True),
    )
    row_piece = lax.all_gather(normed, "tp", axis=0, tiled=True)
    queries_part = jnp.dot(row_piece, wq_full, preferred_element_type=jnp.float32).astype(
        jnp.bfloat16
    )
    keys_part = (
        jnp.dot(row_piece, wk_full, preferred_element_type=jnp.float32) * key_scale
    ).astype(jnp.bfloat16)
    values_part = jnp.dot(row_piece, wv_full, preferred_element_type=jnp.float32).astype(
        jnp.bfloat16
    )
    gate_part = jnp.dot(row_piece, gate_cols, preferred_element_type=jnp.float32)
    group_len = queries_part.shape[0]
    blocks = group_len // BLOCK
    log_input = gate_part[:, :local_heads]
    forget_pre = gate_part[:, local_heads:] + lax.dynamic_slice_in_dim(
        forget_bias, first_head, local_heads, 0
    )
    log_forget = jax.nn.log_sigmoid(
        forget_pre + lax.dynamic_slice_in_dim(gate_drift, first_head, local_heads, 1)
    )
    query_blk = queries_part.reshape(blocks, BLOCK, local_heads, key_width)
    key_blk = keys_part.reshape(blocks, BLOCK, local_heads, key_width)
    value_blk = values_part.reshape(blocks, BLOCK, local_heads, value_width)
    input_blk = log_input.reshape(blocks, BLOCK, local_heads).transpose(0, 2, 1)
    forget_blk = log_forget.reshape(blocks, BLOCK, local_heads).transpose(0, 2, 1)
    within = jnp.cumsum(forget_blk, axis=2)
    causal = jnp.arange(BLOCK)[:, None] >= jnp.arange(BLOCK)[None, :]
    log_pair = jnp.where(
        causal, within[..., :, None] - within[..., None, :] + input_blk[..., None, :], -jnp.inf
    )
    peak_intra = jnp.max(log_pair, axis=3)
    scores = jnp.einsum("nshd,nrhd->nhsr", query_blk, key_blk, preferred_element_type=jnp.float32)
    weights = scores * jnp.exp(log_pair - peak_intra[..., None])
    numer_intra = jnp.einsum(
        "nhsr,nrhv->nhsv",
        weights.astype(jnp.bfloat16),
        value_blk,
        preferred_element_type=jnp.float32,
    )
    denom_intra = jnp.sum(weights, axis=3)
    span_log = within[..., -1]
    log_write = span_log[..., None] - within + input_blk
    span_top = jnp.max(log_write, axis=2)
    write_scale = jnp.exp(log_write - span_top[..., None])
    key_scaled = key_blk.astype(jnp.float32) * write_scale.transpose(0, 2, 1)[..., None]
    value_wide = value_blk.astype(jnp.float32)
    span_mat = jnp.einsum("nrhv,nrhd->nhvd", value_wide, key_scaled, precision=highest)
    span_vec = jnp.sum(key_scaled, axis=1)
    summary = (span_log, span_top, span_mat, span_vec)
    empty_state = (
        jnp.zeros((local_heads, value_width, key_width), jnp.float32),
        jnp.zeros((local_heads, key_width), jnp.float32),
        jnp.full((local_heads,), lowest_log, jnp.float32),
    )
    local_end, local_starts = prefix_states(empty_state, summary)
    device_summary = (jnp.sum(span_log, axis=0),) + local_end
    identity_all = (jnp.zeros((local_heads,), jnp.float32),) + empty_state
    incoming = prefix(device_summary, "sp", join_devices, identity_all)
    query_wide = query_blk.astype(jnp.float32)
    intra_part = (numer_intra, denom_intra, peak_intra)
    start_mat, start_vec, start_top = local_starts
    local_part = (
        jnp.einsum("nhvd,nshd->nhsv", start_mat, query_wide, precision=highest),
        jnp.einsum("nhd,nshd->nhs", start_vec, query_wide, precision=highest),
        within + start_top[..., None],
    )
    numerator, denominator, peak_log = blend_parts(local_part, intra_part)
    entry_log, entry_mat, entry_vec, entry_top = incoming
    before_log = jnp.concatenate(
        [jnp.zeros((1, local_heads), jnp.float32), jnp.cumsum(span_log, axis=0)[:-1]], axis=0
    )
    from_left = (
        jnp.einsum("hvd,nshd->nhsv", entry_mat, query_wide, precision=highest),
        jnp.einsum("hd,nshd->nhs", entry_vec, query_wide, precision=highest),
        within + (before_log + entry_top[None, :])[..., None],
    )
    numerator, denominator, peak_log = blend_parts((numerator, denominator, peak_log), from_left)
    hidden = numerator / jnp.maximum(jnp.abs(denominator), jnp.exp(-peak_log))[..., None]
    hidden = hidden.transpose(0, 2, 1, 3).reshape(group_len, local_heads, value_width)
    head_gains = lax.dynamic_slice_in_dim(
        head_gain, first_head * value_width, local_heads * value_width, 0
    )
    head_gains = head_gains.astype(jnp.float32).reshape(local_heads, value_width)
    normed_heads = (
        hidden
        * lax.rsqrt(jnp.mean(hidden * hidden, axis=2, keepdims=True) + norm_floor)
        * head_gains
    )
    normed_heads = normed_heads.astype(jnp.bfloat16).reshape(group_len, local_heads * value_width)
    out_slab = lax.all_gather(w_out, "sp", axis=0, tiled=True)
    return lax.psum_scatter(
        lax.dot_general(
            normed_heads, out_slab, (((1,), (1,)), ((), ())), preferred_element_type=jnp.float32
        ).astype(jnp.bfloat16),
        "tp",
        scatter_dimension=0,
        tiled=True,
    )


ring_limit = 16
drift_span = 128
MESH = pl.DeviceIdType.MESH
f32 = jnp.float32
bf16 = jnp.bfloat16


def dot_nt(a, b):
    return lax.dot_general(a, b, (((1,), (1,)), ((), ())), preferred_element_type=f32)


def when(flag):
    return flag.astype(jnp.int32).astype(f32)


def square_kernel(
    n,
    tp,
    tokens,
    pre_gain,
    w_query,
    w_key,
    w_value,
    w_igate,
    w_fgate,
    forget_bias,
    drift,
    head_gain,
    w_out,
    out,
    tok_all,
    drift_in,
    normed,
    own_key,
    own_value,
    own_query,
    own_out,
    key_in,
    value_in,
    query_in,
    out_in,
    state_own,
    state_in,
    aux_own,
    aux_in,
    acc,
    heads,
    shares,
    pair_in,
    pair_sum,
    far_in,
    final_sum,
    shares_in,
    tok_send,
    tok_recv,
    drift_send,
    drift_recv,
    near_send,
    near_recv,
    far_send,
    far_recv,
    first_sems,
    first_recv,
    ring_send,
    ring_recv,
    state_send,
    state_recv,
    aux_send,
    aux_recv,
    pair_send,
    pair_recv,
    sum_send,
    sum_recv,
    share_send,
    share_recv,
):
    s = lax.axis_index("sp")
    t = lax.axis_index("tp")
    q = n // 2
    steps = q - 1
    zh = s // q
    r = s % q
    y = t // 2
    c = t % 2
    near = 2 * y + 1 - c
    head = 2 * (2 * y + zh) + c
    rows = tokens.shape[0]
    span_rows = rows * tp
    length = 2 * span_rows
    dk = w_query.shape[1] // 2
    dv = w_value.shape[1] // 2
    depth = w_query.shape[0]
    half = depth // 2
    half_ring = q // 2
    odd = r % 2
    pos = odd * (q - 1) + (1 - 2 * odd) * (r // 2)

    def owner_at(p):
        p = lax.rem(p + 2 * q, q)
        far = p // half_ring
        return far * (2 * (q - 1 - p) + 1) + (1 - far) * 2 * p

    targets = (zh * q + owner_at(pos + 1), zh * q + owner_at(pos - 1))

    barrier = pltpu.get_barrier_semaphore()
    me = s * tp + t
    for i in range(1, n * tp):
        other = lax.rem(me + i, n * tp)
        pl.semaphore_signal(
            barrier,
            inc=1,
            device_id={"sp": other // tp, "tp": lax.rem(other, tp)},
            device_id_type=MESH,
        )
    pl.semaphore_wait(barrier, n * tp - 1)

    copies = []
    guarded = []

    def remote(source, target, send, recv, sp_at, tp_at):
        return pltpu.make_async_remote_copy(
            src_ref=source,
            dst_ref=target,
            send_sem=send,
            recv_sem=recv,
            device_id={"sp": sp_at, "tp": tp_at},
            device_id_type=MESH,
        )

    def send(*args):
        copy = remote(*args)
        copy.start()
        copies.append(copy)
        return copy

    def send_or_keep(source, target, send_sem, recv_sem, sp_at, tp_at):
        away = (sp_at != s) | (tp_at != t)
        copy = remote(source, target, send_sem, recv_sem, sp_at, tp_at)

        @pl.when(away)
        def _():
            copy.start()

        @pl.when(jnp.logical_not(away))
        def _():
            pltpu.make_async_copy(source, target, recv_sem).start()

        guarded.append((away, copy))
        return copy

    def arrived(target, sem):
        pltpu.make_async_copy(target, target, sem).wait()

    pieces = (
        (0, w_key, own_key, key_in),
        (1, w_value, own_value, value_in),
        (2, w_query, own_query, query_in),
        (3, w_out, own_out, out_in),
    )
    stays = zh == c
    def first_send(p):
        _, own, stage, _ = pieces[p]
        width = own.shape[1] // 2
        for g in range(2):
            mine = own.at[:, pl.ds(g * width, width)]
            keep = stays & (c == g)
            block = (zh + c) % 2
            copy = remote(
                mine,
                stage.at[block],
                first_sems.at[g, p],
                first_recv.at[block, p],
                c * q + r,
                2 * y + g,
            )

            @pl.when(jnp.logical_not(keep))
            def _():
                copy.start()

            @pl.when(keep)
            def _():
                pltpu.make_async_copy(mine, stage.at[0], first_recv.at[0, p]).start()

            guarded.append((jnp.logical_not(keep), copy))

    for p in range(3):
        first_send(p)

    def ring_copy(p, block, d, k):
        _, _, stage, landing = pieces[p]
        size = stage.shape[1] // 2
        source = (
            stage.at[block, pl.ds(d * size, size)] if k == 0 else landing.at[block, d, k - 1]
        )
        return send(
            source,
            landing.at[block, d, k],
            ring_send.at[p, block, d, k],
            ring_recv.at[p, block, d, k],
            targets[d],
            t,
        )

    live = {}

    def ring_start(p, block):
        arrived(pieces[p][2].at[block], first_recv.at[block, p])
        for d in range(2):
            live[p, block, d] = ring_copy(p, block, d, 0)

    def ring_step(p, block, k):
        for d in range(2):
            live[p, block, d].wait_recv()
            if k + 1 < steps:
                live[p, block, d] = ring_copy(p, block, d, k + 1)

    cols = (slice(0, dk), slice(dk, dk + dv), slice(dk + dv, 2 * dk + dv))

    def origin(block, owner):
        return (zh if block == 0 else 1 - zh) * q + owner

    def own_product(block, fresh):
        at = pl.ds(pl.multiple_of(origin(block, r) * depth, depth), depth)
        part = normed[:, at]
        for p in range(3):
            product = jnp.dot(part, pieces[p][2][block], preferred_element_type=f32)
            acc[:, cols[p]] = product if fresh else acc[:, cols[p]] + product

    def step_product(block, k):
        for d in range(2):
            owner = owner_at(pos - 1 - k) if d == 0 else owner_at(pos + 1 + k)
            at = pl.ds(
                pl.multiple_of(origin(block, owner) * depth + d * half, half), half
            )
            part = normed[:, at]
            for p in range(3):
                acc[:, cols[p]] += jnp.dot(
                    part, pieces[p][3][block, d, k], preferred_element_type=f32
                )

    for p in range(3):
        ring_start(p, 0)
    half_tp = tp // 2
    x = s % 2
    row_at = pl.ds(pl.multiple_of(x * span_rows + t * rows, rows), rows)

    def tokens_at(xx, to_t):
        start = pl.multiple_of(xx * span_rows + to_t * rows, rows)
        return tok_all.at[pl.ds(start, rows)]

    for p in range(3):
        ring_step(p, 0, 0)
    for g in range(2):
        to_s = g * q + s // 2
        send_or_keep(
            tokens, tok_all.at[row_at], tok_send.at[g], tok_recv.at[x], to_s, t
        )
        send_or_keep(
            drift, drift_in.at[x], drift_send.at[g], drift_recv.at[x], to_s, t
        )
    for k in range(1, steps):
        for p in range(3):
            ring_step(p, 0, k)
    first_send(3)
    for p in range(3):
        ring_start(p, 1)
    for xx in range(2):
        block = tokens_at(xx, t)
        arrived(block, tok_recv.at[xx])
        arrived(drift_in.at[xx], drift_recv.at[xx])
        for i in range(1, half_tp):
            far_t = 2 * lax.rem(y + i, half_tp) + c
            send(block, block, far_send.at[xx, i - 1], far_recv.at[xx, i - 1], s, far_t)
        send(block, block, near_send.at[xx, 0], near_recv.at[xx, 0], s, near)
    for p in range(3):
        ring_step(p, 1, 0)
    for xx in range(2):
        for i in range(1, half_tp):
            block = tokens_at(xx, 2 * lax.rem(y - i + half_tp, half_tp) + c)
            arrived(block, far_recv.at[xx, i - 1])
            send(block, block, near_send.at[xx, i], near_recv.at[xx, i], s, near)
    for k in range(1, steps - 1):
        for p in range(3):
            ring_step(p, 1, k)
    ring_start(3, 0)
    for xx in range(2):
        for i in range(half_tp):
            block = tokens_at(xx, 2 * lax.rem(y - i + half_tp, half_tp) + 1 - c)
            arrived(block, near_recv.at[xx, i])
    wide = tok_all[...].astype(f32)
    scale = lax.rsqrt(jnp.mean(wide * wide, axis=1, keepdims=True) + norm_floor)
    normed[...] = (wide * scale * pre_gain[...].astype(f32)[None, :]).astype(bf16)

    own_product(0, True)
    for k in range(steps):
        step_product(0, k)
    ring_step(3, 0, 0)
    ring_start(3, 1)
    own_product(1, False)
    for k in range(steps - 1):
        step_product(1, k)
    all_normed = normed[...]
    gate_in = dot_nt(all_normed, w_igate[...])
    gate_forget = dot_nt(all_normed, w_fgate[...])
    row_id = lax.broadcasted_iota(jnp.int32, (length, length), 0)
    col_id = lax.broadcasted_iota(jnp.int32, (length, length), 1)
    causal = row_id >= col_id
    pick = lax.broadcasted_iota(jnp.int32, gate_in.shape, 1) == head
    late = lax.broadcasted_iota(jnp.int32, (length, 1), 0) >= span_rows
    mine = pl.ds(head, 1)
    offset = jnp.where(late, drift_in[1, mine, :][:, :1], drift_in[0, mine, :][:, :1])
    forget_pre = (
        jnp.sum(jnp.where(pick, gate_forget, 0.0), axis=1, keepdims=True)
        + forget_bias[head]
        + offset
    )
    lf_col = jnp.minimum(forget_pre, 0.0) - jnp.log1p(jnp.exp(-jnp.abs(forget_pre)))
    in_col = jnp.sum(jnp.where(pick, gate_in, 0.0), axis=1, keepdims=True)
    lf_row = jnp.sum(jnp.where(row_id == col_id, lf_col, 0.0), axis=0, keepdims=True)
    in_row = jnp.sum(jnp.where(row_id == col_id, in_col, 0.0), axis=0, keepdims=True)
    b_col = jnp.sum(jnp.where(causal, lf_row, 0.0), axis=1, keepdims=True)
    b_row = jnp.sum(jnp.where(row_id <= col_id, lf_col, 0.0), axis=0, keepdims=True)
    span = jnp.sum(lf_col, axis=0, keepdims=True)
    write = span - b_col + in_col
    top = jnp.max(write, axis=0, keepdims=True)
    write_scale = jnp.exp(write - top)
    log_pair = jnp.where(causal, b_col - b_row + in_row, lowest_log)
    peak = jnp.max(log_pair, axis=1, keepdims=True)
    decay = jnp.where(causal, jnp.exp(log_pair - peak), 0.0)

    for p in range(3):
        ring_step(p, 1, steps - 1)
    step_product(1, steps - 1)
    keys = (acc[:, cols[0]] * (dk**-0.5)).astype(bf16)
    values = acc[:, cols[1]].astype(bf16)
    queries = acc[:, cols[2]].astype(bf16)
    key_scaled = keys.astype(f32) * write_scale
    state_own[...] = jnp.dot(
        key_scaled.T.astype(bf16), values, preferred_element_type=f32
    ).astype(bf16)
    aux_own[0:1, :] = jnp.broadcast_to(span, (1, dk))
    aux_own[1:2, :] = jnp.broadcast_to(top, (1, dk))
    aux_own[2:3, :] = jnp.sum(key_scaled, axis=0, keepdims=True)
    aux_own[3:, :] = jnp.zeros((aux_own.shape[0] - 3, dk), f32)
    state_copies = []
    for i in range(1, q):
        peer = zh * q + lax.rem(r + i, q)
        state_copies.append(
            (
                send(
                    state_own,
                    state_in.at[i - 1],
                    state_send.at[i - 1],
                    state_recv.at[i - 1],
                    peer,
                    t,
                ),
                send(
                    aux_own,
                    aux_in.at[i - 1],
                    aux_send.at[i - 1],
                    aux_recv.at[i - 1],
                    peer,
                    t,
                ),
            )
        )
    weights = dot_nt(queries, keys) * decay
    numer = jnp.dot(weights.astype(bf16), values, preferred_element_type=f32)
    denom = jnp.sum(weights, axis=1, keepdims=True)
    ring_step(3, 0, 1)
    ring_step(3, 1, 0)
    for pair in state_copies:
        for copy in pair:
            copy.wait_recv()
    owners = [lax.rem(r - i + q, q) for i in range(1, q)]
    logs = []
    for k in range(steps):
        total = aux_in[k, 1:2, :]
        for i in range(steps):
            if i != k:
                between = when((owners[i] > owners[k]) & (owners[i] < r))
                total = total + between * aux_in[i, 0:1, :]
        before = when(owners[k] < r)
        logs.append((before, before * total + (1.0 - before) * lowest_log))
    entry = functools.reduce(jnp.maximum, [log for _, log in logs])
    mat = jnp.zeros((dk, dv), f32)
    vec = jnp.zeros((1, dk), f32)
    for k in range(steps):
        before, log = logs[k]
        weight = before * jnp.exp(log - entry)
        mat = mat + weight[:, :1] * state_in[k].astype(f32)
        vec = vec + weight * aux_in[k, 2:3, :]
    carried = b_col + entry[:, :1]
    new_top = jnp.maximum(peak, carried)
    w_intra = jnp.exp(peak - new_top)
    w_carry = jnp.exp(carried - new_top)
    numer = w_intra * numer + w_carry * jnp.dot(
        queries, mat.astype(bf16), preferred_element_type=f32
    )
    denom = w_intra * denom + w_carry * jnp.sum(
        queries.astype(f32) * vec, axis=1, keepdims=True
    )
    hidden = numer / jnp.maximum(jnp.abs(denom), jnp.exp(-new_top))
    gain = head_gain[pl.ds(pl.multiple_of(head * dv, dv), dv)].astype(f32)[None, :]
    heads[...] = (
        hidden
        * lax.rsqrt(jnp.mean(hidden * hidden, axis=1, keepdims=True) + norm_floor)
        * gain
    ).astype(bf16)

    ready = heads[...]
    e_depth = w_out.shape[0]
    e_half = e_depth // 2
    wide_half = q * e_depth
    theirs = pl.ds(pl.multiple_of((1 - c) * span_rows, span_rows), span_rows)
    kept = pl.ds(pl.multiple_of(c * span_rows, span_rows), span_rows)

    def share_own(block):
        at = pl.ds(pl.multiple_of(r * e_depth, e_depth), e_depth)
        shares[block, :, at] = dot_nt(ready, own_out[block]).astype(bf16)

    def share_step(block, k):
        for d in range(2):
            owner = owner_at(pos - 1 - k) if d == 0 else owner_at(pos + 1 + k)
            at = pl.ds(pl.multiple_of(owner * e_depth + d * e_half, e_half), e_half)
            shares[block, :, at] = dot_nt(ready, out_in[block, d, k]).astype(bf16)

    def pair_start(block):
        return send(
            shares.at[block, theirs],
            pair_in.at[block],
            pair_send.at[block],
            pair_recv.at[block],
            s,
            near,
        )

    def far_start(block, pair):
        pair.wait_recv()
        pair_sum[block] = (
            shares[block, kept, :].astype(f32) + pair_in[block].astype(f32)
        ).astype(bf16)
        found = []
        for i in range(1, half_tp):
            yy = lax.rem(y + i, half_tp)
            at = pl.ds(pl.multiple_of(yy * 2 * rows, 2 * rows), 2 * rows)
            found.append(
                send(
                    pair_sum.at[block, at],
                    far_in.at[block, i - 1],
                    sum_send.at[block, i - 1],
                    sum_recv.at[block, i - 1],
                    s,
                    2 * yy + c,
                )
            )
        return found

    def share_out(block, found):
        at = pl.ds(pl.multiple_of(y * 2 * rows, 2 * rows), 2 * rows)
        total = pair_sum[block, at, :].astype(f32)
        for i, copy in enumerate(found):
            copy.wait_recv()
            total = total + far_in[block, i].astype(f32)
        final_sum[block] = total.astype(bf16)
        side = zh if block == 0 else 1 - zh
        for cc in range(2):
            send_or_keep(
                final_sum.at[block, pl.ds(cc * rows, rows)],
                shares_in.at[zh, side],
                share_send.at[block, cc],
                share_recv.at[zh, side],
                2 * r + c,
                2 * y + cc,
            )

    share_own(0)
    for k in range(steps):
        if k > 1:
            ring_step(3, 0, k)
        share_step(0, k)
    pair = pair_start(0)
    share_own(1)
    for k in range(steps - 1):
        if k > 0:
            ring_step(3, 1, k)
        share_step(1, k)
    found = far_start(0, pair)
    ring_step(3, 1, steps - 1)
    share_step(1, steps - 1)
    pair = pair_start(1)
    share_out(0, found)
    found = far_start(1, pair)
    share_out(1, found)
    for side in range(2):
        total = jnp.zeros((rows, wide_half), f32)
        for g in range(2):
            arrived(shares_in.at[g, side], share_recv.at[g, side])
            total = total + shares_in[g, side].astype(f32)
        out[:, side * wide_half : (side + 1) * wide_half] = total.astype(bf16)
    for copy in copies:
        copy.wait_send()
    for away, copy in guarded:

        @pl.when(away)
        def _():
            copy.wait_send()


def on_device_ring(
    n,
    tp,
    tokens,
    pre_gain,
    w_query,
    w_key,
    w_value,
    w_igate,
    w_fgate,
    forget_bias,
    gate_drift,
    head_gain,
    w_out,
):
    heads = w_igate.shape[1]
    if heads != 2 * tp or gate_drift.shape[0] > drift_span:
        return on_device(
            tokens,
            pre_gain,
            w_query,
            w_key,
            w_value,
            w_igate,
            w_fgate,
            forget_bias,
            gate_drift,
            head_gain,
            w_out,
        )
    rows, width = tokens.shape
    length = 2 * rows * tp
    q = n // 2
    steps = q - 1
    half_tp = tp // 2
    dk = w_query.shape[1] // 2
    dv = w_value.shape[1] // 2
    features = w_out.shape[0] * n
    vmem = pl.BlockSpec(memory_space=pltpu.VMEM)
    dma = pltpu.SemaphoreType.DMA
    weights = (w_key, w_value, w_query, w_out)
    smem = pl.BlockSpec(memory_space=pltpu.SMEM)
    return pl.pallas_call(
        functools.partial(square_kernel, n, tp),
        out_shape=jax.ShapeDtypeStruct((rows, features), bf16),
        in_specs=[vmem] * 7 + [smem] + [vmem] * 3,
        out_specs=vmem,
        scratch_shapes=[
            pltpu.VMEM((length, width), bf16),
            pltpu.VMEM((2, heads, gate_drift.shape[0]), f32),
            pltpu.VMEM((length, width), bf16),
            *[pltpu.VMEM((2, w.shape[0], w.shape[1] // 2), bf16) for w in weights],
            *[
                pltpu.VMEM((2, 2, steps, w.shape[0] // 2, w.shape[1] // 2), bf16)
                for w in weights
            ],
            pltpu.VMEM((dk, dv), bf16),
            pltpu.VMEM((steps, dk, dv), bf16),
            pltpu.VMEM((8, dk), f32),
            pltpu.VMEM((steps, 8, dk), f32),
            pltpu.VMEM((length, 2 * dk + dv), f32),
            pltpu.VMEM((length, dv), bf16),
            pltpu.VMEM((2, length, features // 2), bf16),
            pltpu.VMEM((2, length // 2, features // 2), bf16),
            pltpu.VMEM((2, length // 2, features // 2), bf16),
            pltpu.VMEM((2, half_tp - 1, 2 * rows, features // 2), bf16),
            pltpu.VMEM((2, 2 * rows, features // 2), bf16),
            pltpu.VMEM((2, 2, rows, features // 2), bf16),
            dma((2,)),
            dma((2,)),
            dma((2,)),
            dma((2,)),
            dma((2, half_tp)),
            dma((2, half_tp)),
            dma((2, half_tp)),
            dma((2, half_tp)),
            dma((2, 4)),
            dma((2, 4)),
            dma((4, 2, 2, steps)),
            dma((4, 2, 2, steps)),
            dma((steps,)),
            dma((steps,)),
            dma((steps,)),
            dma((steps,)),
            dma((2,)),
            dma((2,)),
            dma((2, half_tp)),
            dma((2, half_tp)),
            dma((2, 2)),
            dma((2, 2)),
        ],
        compiler_params=pltpu.CompilerParams(collective_id=0, has_side_effects=True),
    )(
        tokens,
        pre_gain,
        w_query,
        w_key,
        w_value,
        w_igate.T,
        w_fgate.T,
        forget_bias,
        gate_drift.T,
        head_gain,
        w_out,
    )


def solution(mesh):
    in_specs = (
        P(("sp", "tp"), None),
        P(),
        P("sp", "tp"),
        P("sp", "tp"),
        P("sp", "tp"),
        P(),
        P(),
        P(),
        P("sp", None),
        P(),
        P("sp", "tp"),
    )
    out_specs = P(("sp", "tp"), None)
    body = on_device
    if mesh.shape["sp"] <= ring_limit and mesh.shape["sp"] % 4 == 0 and mesh.shape["tp"] % 4 == 0:
        body = functools.partial(on_device_ring, mesh.shape["sp"], mesh.shape["tp"])
    return jax.shard_map(
        body, mesh=mesh, in_specs=in_specs, out_specs=out_specs, check_vma=False
    )
```

```python
import functools

import jax
import jax.numpy as jnp
from jax import lax
from jax.experimental import pallas as pl
from jax.experimental.pallas import tpu as pltpu
from jax.sharding import PartitionSpec as P

BLOCK = 64


norm_floor = 0.1
lowest_log = -1e30
highest = lax.Precision.HIGHEST


def prefix(value, axis, combine, identity):
    peers, position = (lax.axis_size(axis), lax.axis_index(axis))
    everything = jax.tree.map(
        lambda part, kind: lax.all_gather(part.astype(kind), axis),
        value,
        jax.tree.map(lambda a: jnp.bfloat16 if a.dtype == jnp.float32 else a.dtype, value),
    )
    start = jax.tree.map(
        lambda part, zero: jnp.broadcast_to(jnp.asarray(zero, part.dtype), part.shape),
        value,
        identity,
    )

    def step(k, before):
        reached = k < position
        new = combine(
            before, jax.tree.map(lambda part, own: part[k].astype(own.dtype), everything, value)
        )
        return jax.tree.map(lambda a, b: jnp.where(reached, a, b), new, before)

    return lax.fori_loop(0, peers, step, start)


def advance(memory, summary):
    old_mat, old_vec, old_top = memory
    span_log, span_top, span_mat, span_vec = summary
    new_top = jnp.maximum(span_log + old_top, span_top)
    kept_part = jnp.exp(span_log + old_top - new_top)
    fresh_part = jnp.exp(span_top - new_top)
    return (
        kept_part[:, None, None] * old_mat + fresh_part[:, None, None] * span_mat,
        kept_part[:, None] * old_vec + fresh_part[:, None] * span_vec,
        new_top,
    )


def prefix_states(initial, summary):

    def stepper(memory, one_block):
        return (advance(memory, one_block), memory)

    return lax.scan(stepper, initial, summary)


def join_devices(earlier, later_part):
    early_log, early_mat, early_vec, early_top = earlier
    late_log, late_mat, late_vec, late_top = later_part
    new_top = jnp.maximum(late_log + early_top, late_top)
    kept_part = jnp.exp(late_log + early_top - new_top)
    fresh_part = jnp.exp(late_top - new_top)
    return (
        early_log + late_log,
        kept_part[:, None, None] * early_mat + fresh_part[:, None, None] * late_mat,
        kept_part[:, None] * early_vec + fresh_part[:, None] * late_vec,
        new_top,
    )


def blend_parts(first_part, second_part):
    numer_first, denom_first, peak_first = first_part
    numer_second, denom_second, peak_second = second_part
    new_top = jnp.maximum(peak_first, peak_second)
    weight_first = jnp.exp(peak_first - new_top)
    weight_second = jnp.exp(peak_second - new_top)
    return (
        weight_first[..., None] * numer_first + weight_second[..., None] * numer_second,
        weight_first * denom_first + weight_second * denom_second,
        new_top,
    )


def on_device(
    tokens,
    pre_gain,
    w_query,
    w_key,
    w_value,
    w_igate,
    w_fgate,
    forget_bias,
    gate_drift,
    head_gain,
    w_out,
):
    tp_size = lax.axis_size("tp")
    head_count = w_igate.shape[1]
    local_heads = head_count // tp_size
    first_head = lax.axis_index("tp") * local_heads
    key_width = w_query.shape[1] // local_heads
    value_width = w_value.shape[1] // local_heads
    token_wide = tokens.astype(jnp.float32)
    scaled = token_wide * lax.rsqrt(
        jnp.mean(token_wide * token_wide, axis=1, keepdims=True) + norm_floor
    )
    normed = (scaled * pre_gain.astype(jnp.float32)).astype(jnp.bfloat16)
    gate_cols = jnp.concatenate(
        [
            lax.dynamic_slice_in_dim(w_igate, first_head, local_heads, 1),
            lax.dynamic_slice_in_dim(w_fgate, first_head, local_heads, 1),
        ],
        axis=1,
    )
    key_scale = key_width ** (-0.5)
    wq_full, wk_full, wv_full = (
        lax.all_gather(w_query, "sp", axis=0, tiled=True),
        lax.all_gather(w_key, "sp", axis=0, tiled=True),
        lax.all_gather(w_value, "sp", axis=0, tiled=True),
    )
    row_piece = lax.all_gather(normed, "tp", axis=0, tiled=True)
    queries_part = jnp.dot(row_piece, wq_full, preferred_element_type=jnp.float32).astype(
        jnp.bfloat16
    )
    keys_part = (
        jnp.dot(row_piece, wk_full, preferred_element_type=jnp.float32) * key_scale
    ).astype(jnp.bfloat16)
    values_part = jnp.dot(row_piece, wv_full, preferred_element_type=jnp.float32).astype(
        jnp.bfloat16
    )
    gate_part = jnp.dot(row_piece, gate_cols, preferred_element_type=jnp.float32)
    group_len = queries_part.shape[0]
    blocks = group_len // BLOCK
    log_input = gate_part[:, :local_heads]
    forget_pre = gate_part[:, local_heads:] + lax.dynamic_slice_in_dim(
        forget_bias, first_head, local_heads, 0
    )
    log_forget = jax.nn.log_sigmoid(
        forget_pre + lax.dynamic_slice_in_dim(gate_drift, first_head, local_heads, 1)
    )
    query_blk = queries_part.reshape(blocks, BLOCK, local_heads, key_width)
    key_blk = keys_part.reshape(blocks, BLOCK, local_heads, key_width)
    value_blk = values_part.reshape(blocks, BLOCK, local_heads, value_width)
    input_blk = log_input.reshape(blocks, BLOCK, local_heads).transpose(0, 2, 1)
    forget_blk = log_forget.reshape(blocks, BLOCK, local_heads).transpose(0, 2, 1)
    within = jnp.cumsum(forget_blk, axis=2)
    causal = jnp.arange(BLOCK)[:, None] >= jnp.arange(BLOCK)[None, :]
    log_pair = jnp.where(
        causal, within[..., :, None] - within[..., None, :] + input_blk[..., None, :], -jnp.inf
    )
    peak_intra = jnp.max(log_pair, axis=3)
    scores = jnp.einsum("nshd,nrhd->nhsr", query_blk, key_blk, preferred_element_type=jnp.float32)
    weights = scores * jnp.exp(log_pair - peak_intra[..., None])
    numer_intra = jnp.einsum(
        "nhsr,nrhv->nhsv",
        weights.astype(jnp.bfloat16),
        value_blk,
        preferred_element_type=jnp.float32,
    )
    denom_intra = jnp.sum(weights, axis=3)
    span_log = within[..., -1]
    log_write = span_log[..., None] - within + input_blk
    span_top = jnp.max(log_write, axis=2)
    write_scale = jnp.exp(log_write - span_top[..., None])
    key_scaled = key_blk.astype(jnp.float32) * write_scale.transpose(0, 2, 1)[..., None]
    value_wide = value_blk.astype(jnp.float32)
    span_mat = jnp.einsum("nrhv,nrhd->nhvd", value_wide, key_scaled, precision=highest)
    span_vec = jnp.sum(key_scaled, axis=1)
    summary = (span_log, span_top, span_mat, span_vec)
    empty_state = (
        jnp.zeros((local_heads, value_width, key_width), jnp.float32),
        jnp.zeros((local_heads, key_width), jnp.float32),
        jnp.full((local_heads,), lowest_log, jnp.float32),
    )
    local_end, local_starts = prefix_states(empty_state, summary)
    device_summary = (jnp.sum(span_log, axis=0),) + local_end
    identity_all = (jnp.zeros((local_heads,), jnp.float32),) + empty_state
    incoming = prefix(device_summary, "sp", join_devices, identity_all)
    query_wide = query_blk.astype(jnp.float32)
    intra_part = (numer_intra, denom_intra, peak_intra)
    start_mat, start_vec, start_top = local_starts
    local_part = (
        jnp.einsum("nhvd,nshd->nhsv", start_mat, query_wide, precision=highest),
        jnp.einsum("nhd,nshd->nhs", start_vec, query_wide, precision=highest),
        within + start_top[..., None],
    )
    numerator, denominator, peak_log = blend_parts(local_part, intra_part)
    entry_log, entry_mat, entry_vec, entry_top = incoming
    before_log = jnp.concatenate(
        [jnp.zeros((1, local_heads), jnp.float32), jnp.cumsum(span_log, axis=0)[:-1]], axis=0
    )
    from_left = (
        jnp.einsum("hvd,nshd->nhsv", entry_mat, query_wide, precision=highest),
        jnp.einsum("hd,nshd->nhs", entry_vec, query_wide, precision=highest),
        within + (before_log + entry_top[None, :])[..., None],
    )
    numerator, denominator, peak_log = blend_parts((numerator, denominator, peak_log), from_left)
    hidden = numerator / jnp.maximum(jnp.abs(denominator), jnp.exp(-peak_log))[..., None]
    hidden = hidden.transpose(0, 2, 1, 3).reshape(group_len, local_heads, value_width)
    head_gains = lax.dynamic_slice_in_dim(
        head_gain, first_head * value_width, local_heads * value_width, 0
    )
    head_gains = head_gains.astype(jnp.float32).reshape(local_heads, value_width)
    normed_heads = (
        hidden
        * lax.rsqrt(jnp.mean(hidden * hidden, axis=2, keepdims=True) + norm_floor)
        * head_gains
    )
    normed_heads = normed_heads.astype(jnp.bfloat16).reshape(group_len, local_heads * value_width)
    out_slab = lax.all_gather(w_out, "sp", axis=0, tiled=True)
    return lax.psum_scatter(
        lax.dot_general(
            normed_heads, out_slab, (((1,), (1,)), ((), ())), preferred_element_type=jnp.float32
        ).astype(jnp.bfloat16),
        "tp",
        scatter_dimension=0,
        tiled=True,
    )


ring_limit = 16
drift_span = 128
MESH = pl.DeviceIdType.MESH
f32 = jnp.float32
bf16 = jnp.bfloat16


def dot_nt(a, b):
    return lax.dot_general(a, b, (((1,), (1,)), ((), ())), preferred_element_type=f32)


def when(flag):
    return flag.astype(jnp.int32).astype(f32)


def square_kernel(
    n,
    tp,
    tokens,
    pre_gain,
    w_query,
    w_key,
    w_value,
    w_igate,
    w_fgate,
    forget_bias,
    drift,
    head_gain,
    w_out,
    out,
    tok_all,
    drift_in,
    normed,
    own_key,
    own_value,
    own_query,
    own_out,
    key_in,
    value_in,
    query_in,
    out_in,
    state_own,
    state_in,
    aux_own,
    aux_in,
    acc,
    heads,
    shares,
    pair_in,
    pair_sum,
    far_in,
    final_sum,
    shares_in,
    tok_send,
    tok_recv,
    drift_send,
    drift_recv,
    near_send,
    near_recv,
    far_send,
    far_recv,
    first_sems,
    first_recv,
    ring_send,
    ring_recv,
    state_send,
    state_recv,
    aux_send,
    aux_recv,
    pair_send,
    pair_recv,
    sum_send,
    sum_recv,
    share_send,
    share_recv,
):
    s = lax.axis_index("sp")
    t = lax.axis_index("tp")
    q = n // 2
    steps = q - 1
    zh = s // q
    r = s % q
    y = t // 2
    c = t % 2
    near = 2 * y + 1 - c
    head = 2 * (2 * y + zh) + c
    rows = tokens.shape[0]
    span_rows = rows * tp
    length = 2 * span_rows
    dk = w_query.shape[1] // 2
    dv = w_value.shape[1] // 2
    depth = w_query.shape[0]
    half = depth // 2
    half_ring = q // 2
    odd = r % 2
    pos = odd * (q - 1) + (1 - 2 * odd) * (r // 2)

    def owner_at(p):
        p = lax.rem(p + 2 * q, q)
        far = p // half_ring
        return far * (2 * (q - 1 - p) + 1) + (1 - far) * 2 * p

    targets = (zh * q + owner_at(pos + 1), zh * q + owner_at(pos - 1))

    barrier = pltpu.get_barrier_semaphore()
    me = s * tp + t
    for i in range(1, n * tp):
        other = lax.rem(me + i, n * tp)
        pl.semaphore_signal(
            barrier,
            inc=1,
            device_id={"sp": other // tp, "tp": lax.rem(other, tp)},
            device_id_type=MESH,
        )
    pl.semaphore_wait(barrier, n * tp - 1)

    copies = []
    guarded = []

    def remote(source, target, send, recv, sp_at, tp_at):
        return pltpu.make_async_remote_copy(
            src_ref=source,
            dst_ref=target,
            send_sem=send,
            recv_sem=recv,
            device_id={"sp": sp_at, "tp": tp_at},
            device_id_type=MESH,
        )

    def send(*args):
        copy = remote(*args)
        copy.start()
        copies.append(copy)
        return copy

    def send_or_keep(source, target, send_sem, recv_sem, sp_at, tp_at):
        away = (sp_at != s) | (tp_at != t)
        copy = remote(source, target, send_sem, recv_sem, sp_at, tp_at)

        @pl.when(away)
        def _():
            copy.start()

        @pl.when(jnp.logical_not(away))
        def _():
            pltpu.make_async_copy(source, target, recv_sem).start()

        guarded.append((away, copy))
        return copy

    def arrived(target, sem):
        pltpu.make_async_copy(target, target, sem).wait()

    pieces = (
        (0, w_key, own_key, key_in),
        (1, w_value, own_value, value_in),
        (2, w_query, own_query, query_in),
        (3, w_out, own_out, out_in),
    )
    stays = zh == c
    def first_send(p):
        _, own, stage, _ = pieces[p]
        width = own.shape[1] // 2
        for g in range(2):
            mine = own.at[:, pl.ds(g * width, width)]
            keep = stays & (c == g)
            block = (zh + c) % 2
            copy = remote(
                mine,
                stage.at[block],
                first_sems.at[g, p],
                first_recv.at[block, p],
                c * q + r,
                2 * y + g,
            )

            @pl.when(jnp.logical_not(keep))
            def _():
                copy.start()

            @pl.when(keep)
            def _():
                pltpu.make_async_copy(mine, stage.at[0], first_recv.at[0, p]).start()

            guarded.append((jnp.logical_not(keep), copy))

    for p in range(3):
        first_send(p)

    def ring_copy(p, block, d, k):
        _, _, stage, landing = pieces[p]
        size = stage.shape[1] // 2
        source = (
            stage.at[block, pl.ds(d * size, size)] if k == 0 else landing.at[block, d, k - 1]
        )
        return send(
            source,
            landing.at[block, d, k],
            ring_send.at[p, block, d, k],
            ring_recv.at[p, block, d, k],
            targets[d],
            t,
        )

    live = {}

    def ring_start(p, block):
        arrived(pieces[p][2].at[block], first_recv.at[block, p])
        for d in range(2):
            live[p, block, d] = ring_copy(p, block, d, 0)

    def ring_step(p, block, k):
        for d in range(2):
            live[p, block, d].wait_recv()
            if k + 1 < steps:
                live[p, block, d] = ring_copy(p, block, d, k + 1)

    cols = (slice(0, dk), slice(dk, dk + dv), slice(dk + dv, 2 * dk + dv))

    def origin(block, owner):
        return (zh if block == 0 else 1 - zh) * q + owner

    def own_product(block, fresh):
        at = pl.ds(pl.multiple_of(origin(block, r) * depth, depth), depth)
        part = normed[:, at]
        for p in range(3):
            product = jnp.dot(part, pieces[p][2][block], preferred_element_type=f32)
            acc[:, cols[p]] = product if fresh else acc[:, cols[p]] + product

    def step_product(block, k):
        for d in range(2):
            owner = owner_at(pos - 1 - k) if d == 0 else owner_at(pos + 1 + k)
            at = pl.ds(
                pl.multiple_of(origin(block, owner) * depth + d * half, half), half
            )
            part = normed[:, at]
            for p in range(3):
                acc[:, cols[p]] += jnp.dot(
                    part, pieces[p][3][block, d, k], preferred_element_type=f32
                )

    for p in range(3):
        ring_start(p, 0)
    half_tp = tp // 2
    x = s % 2
    row_at = pl.ds(pl.multiple_of(x * span_rows + t * rows, rows), rows)

    def tokens_at(xx, to_t):
        start = pl.multiple_of(xx * span_rows + to_t * rows, rows)
        return tok_all.at[pl.ds(start, rows)]

    for p in range(3):
        ring_step(p, 0, 0)
    for g in range(2):
        to_s = g * q + s // 2
        send_or_keep(
            tokens, tok_all.at[row_at], tok_send.at[g], tok_recv.at[x], to_s, t
        )
        send_or_keep(
            drift, drift_in.at[x], drift_send.at[g], drift_recv.at[x], to_s, t
        )
    for k in range(1, steps):
        for p in range(3):
            ring_step(p, 0, k)
    first_send(3)
    for p in range(3):
        ring_start(p, 1)
    for xx in range(2):
        block = tokens_at(xx, t)
        arrived(block, tok_recv.at[xx])
        arrived(drift_in.at[xx], drift_recv.at[xx])
        for i in range(1, half_tp):
            far_t = 2 * lax.rem(y + i, half_tp) + c
            send(block, block, far_send.at[xx, i - 1], far_recv.at[xx, i - 1], s, far_t)
        send(block, block, near_send.at[xx, 0], near_recv.at[xx, 0], s, near)
    for p in range(3):
        ring_step(p, 1, 0)
    for xx in range(2):
        for i in range(1, half_tp):
            block = tokens_at(xx, 2 * lax.rem(y - i + half_tp, half_tp) + c)
            arrived(block, far_recv.at[xx, i - 1])
            send(block, block, near_send.at[xx, i], near_recv.at[xx, i], s, near)
    for k in range(1, steps - 1):
        for p in range(3):
            ring_step(p, 1, k)
    ring_start(3, 0)
    for xx in range(2):
        for i in range(half_tp):
            block = tokens_at(xx, 2 * lax.rem(y - i + half_tp, half_tp) + 1 - c)
            arrived(block, near_recv.at[xx, i])
    wide = tok_all[...].astype(f32)
    scale = lax.rsqrt(jnp.mean(wide * wide, axis=1, keepdims=True) + norm_floor)
    normed[...] = (wide * scale * pre_gain[...].astype(f32)[None, :]).astype(bf16)

    own_product(0, True)
    for k in range(steps):
        step_product(0, k)
    own_product(1, False)
    for k in range(steps - 1):
        step_product(1, k)
    ring_step(3, 0, 0)
    all_normed = normed[...]
    gate_in = dot_nt(all_normed, w_igate[...])
    gate_forget = dot_nt(all_normed, w_fgate[...])
    row_id = lax.broadcasted_iota(jnp.int32, (length, length), 0)
    col_id = lax.broadcasted_iota(jnp.int32, (length, length), 1)
    causal = row_id >= col_id
    pick = lax.broadcasted_iota(jnp.int32, gate_in.shape, 1) == head
    late = lax.broadcasted_iota(jnp.int32, (length, 1), 0) >= span_rows
    mine = pl.ds(head, 1)
    offset = jnp.where(late, drift_in[1, mine, :][:, :1], drift_in[0, mine, :][:, :1])
    forget_pre = (
        jnp.sum(jnp.where(pick, gate_forget, 0.0), axis=1, keepdims=True)
        + forget_bias[head]
        + offset
    )
    lf_col = jnp.minimum(forget_pre, 0.0) - jnp.log1p(jnp.exp(-jnp.abs(forget_pre)))
    in_col = jnp.sum(jnp.where(pick, gate_in, 0.0), axis=1, keepdims=True)
    lf_row = jnp.sum(jnp.where(row_id == col_id, lf_col, 0.0), axis=0, keepdims=True)
    in_row = jnp.sum(jnp.where(row_id == col_id, in_col, 0.0), axis=0, keepdims=True)
    b_col = jnp.sum(jnp.where(causal, lf_row, 0.0), axis=1, keepdims=True)
    b_row = jnp.sum(jnp.where(row_id <= col_id, lf_col, 0.0), axis=0, keepdims=True)
    span = jnp.sum(lf_col, axis=0, keepdims=True)
    write = span - b_col + in_col
    top = jnp.max(write, axis=0, keepdims=True)
    write_scale = jnp.exp(write - top)
    log_pair = jnp.where(causal, b_col - b_row + in_row, lowest_log)
    peak = jnp.max(log_pair, axis=1, keepdims=True)
    decay = jnp.where(causal, jnp.exp(log_pair - peak), 0.0)

    for p in range(3):
        ring_step(p, 1, steps - 1)
    step_product(1, steps - 1)
    ring_start(3, 1)
    keys = (acc[:, cols[0]] * (dk**-0.5)).astype(bf16)
    values = acc[:, cols[1]].astype(bf16)
    queries = acc[:, cols[2]].astype(bf16)
    key_scaled = keys.astype(f32) * write_scale
    state_own[...] = jnp.dot(
        key_scaled.T.astype(bf16), values, preferred_element_type=f32
    ).astype(bf16)
    aux_own[0:1, :] = jnp.broadcast_to(span, (1, dk))
    aux_own[1:2, :] = jnp.broadcast_to(top, (1, dk))
    aux_own[2:3, :] = jnp.sum(key_scaled, axis=0, keepdims=True)
    aux_own[3:, :] = jnp.zeros((aux_own.shape[0] - 3, dk), f32)
    state_copies = []
    for i in range(1, q):
        peer = zh * q + lax.rem(r + i, q)
        state_copies.append(
            (
                send(
                    state_own,
                    state_in.at[i - 1],
                    state_send.at[i - 1],
                    state_recv.at[i - 1],
                    peer,
                    t,
                ),
                send(
                    aux_own,
                    aux_in.at[i - 1],
                    aux_send.at[i - 1],
                    aux_recv.at[i - 1],
                    peer,
                    t,
                ),
            )
        )
    weights = dot_nt(queries, keys) * decay
    numer = jnp.dot(weights.astype(bf16), values, preferred_element_type=f32)
    denom = jnp.sum(weights, axis=1, keepdims=True)
    ring_step(3, 0, 1)
    ring_step(3, 1, 0)
    for pair in state_copies:
        for copy in pair:
            copy.wait_recv()
    owners = [lax.rem(r - i + q, q) for i in range(1, q)]
    logs = []
    for k in range(steps):
        total = aux_in[k, 1:2, :]
        for i in range(steps):
            if i != k:
                between = when((owners[i] > owners[k]) & (owners[i] < r))
                total = total + between * aux_in[i, 0:1, :]
        before = when(owners[k] < r)
        logs.append((before, before * total + (1.0 - before) * lowest_log))
    entry = functools.reduce(jnp.maximum, [log for _, log in logs])
    mat = jnp.zeros((dk, dv), f32)
    vec = jnp.zeros((1, dk), f32)
    for k in range(steps):
        before, log = logs[k]
        weight = before * jnp.exp(log - entry)
        mat = mat + weight[:, :1] * state_in[k].astype(f32)
        vec = vec + weight * aux_in[k, 2:3, :]
    carried = b_col + entry[:, :1]
    new_top = jnp.maximum(peak, carried)
    w_intra = jnp.exp(peak - new_top)
    w_carry = jnp.exp(carried - new_top)
    numer = w_intra * numer + w_carry * jnp.dot(
        queries, mat.astype(bf16), preferred_element_type=f32
    )
    denom = w_intra * denom + w_carry * jnp.sum(
        queries.astype(f32) * vec, axis=1, keepdims=True
    )
    hidden = numer / jnp.maximum(jnp.abs(denom), jnp.exp(-new_top))
    gain = head_gain[pl.ds(pl.multiple_of(head * dv, dv), dv)].astype(f32)[None, :]
    heads[...] = (
        hidden
        * lax.rsqrt(jnp.mean(hidden * hidden, axis=1, keepdims=True) + norm_floor)
        * gain
    ).astype(bf16)

    ready = heads[...]
    e_depth = w_out.shape[0]
    e_half = e_depth // 2
    wide_half = q * e_depth
    theirs = pl.ds(pl.multiple_of((1 - c) * span_rows, span_rows), span_rows)
    kept = pl.ds(pl.multiple_of(c * span_rows, span_rows), span_rows)

    def share_own(block):
        at = pl.ds(pl.multiple_of(r * e_depth, e_depth), e_depth)
        shares[block, :, at] = dot_nt(ready, own_out[block]).astype(bf16)

    def share_step(block, k):
        for d in range(2):
            owner = owner_at(pos - 1 - k) if d == 0 else owner_at(pos + 1 + k)
            at = pl.ds(pl.multiple_of(owner * e_depth + d * e_half, e_half), e_half)
            shares[block, :, at] = dot_nt(ready, out_in[block, d, k]).astype(bf16)

    def pair_start(block):
        return send(
            shares.at[block, theirs],
            pair_in.at[block],
            pair_send.at[block],
            pair_recv.at[block],
            s,
            near,
        )

    def far_start(block, pair):
        pair.wait_recv()
        pair_sum[block] = (
            shares[block, kept, :].astype(f32) + pair_in[block].astype(f32)
        ).astype(bf16)
        found = []
        for i in range(1, half_tp):
            yy = lax.rem(y + i, half_tp)
            at = pl.ds(pl.multiple_of(yy * 2 * rows, 2 * rows), 2 * rows)
            found.append(
                send(
                    pair_sum.at[block, at],
                    far_in.at[block, i - 1],
                    sum_send.at[block, i - 1],
                    sum_recv.at[block, i - 1],
                    s,
                    2 * yy + c,
                )
            )
        return found

    def share_out(block, found):
        at = pl.ds(pl.multiple_of(y * 2 * rows, 2 * rows), 2 * rows)
        total = pair_sum[block, at, :].astype(f32)
        for i, copy in enumerate(found):
            copy.wait_recv()
            total = total + far_in[block, i].astype(f32)
        final_sum[block] = total.astype(bf16)
        side = zh if block == 0 else 1 - zh
        for cc in range(2):
            send_or_keep(
                final_sum.at[block, pl.ds(cc * rows, rows)],
                shares_in.at[zh, side],
                share_send.at[block, cc],
                share_recv.at[zh, side],
                2 * r + c,
                2 * y + cc,
            )

    share_own(0)
    for k in range(steps):
        if k > 1:
            ring_step(3, 0, k)
        share_step(0, k)
    pair = pair_start(0)
    share_own(1)
    for k in range(steps - 1):
        if k > 0:
            ring_step(3, 1, k)
        share_step(1, k)
    found = far_start(0, pair)
    ring_step(3, 1, steps - 1)
    share_step(1, steps - 1)
    pair = pair_start(1)
    share_out(0, found)
    found = far_start(1, pair)
    share_out(1, found)
    for side in range(2):
        total = jnp.zeros((rows, wide_half), f32)
        for g in range(2):
            arrived(shares_in.at[g, side], share_recv.at[g, side])
            total = total + shares_in[g, side].astype(f32)
        out[:, side * wide_half : (side + 1) * wide_half] = total.astype(bf16)
    for copy in copies:
        copy.wait_send()
    for away, copy in guarded:

        @pl.when(away)
        def _():
            copy.wait_send()


def on_device_ring(
    n,
    tp,
    tokens,
    pre_gain,
    w_query,
    w_key,
    w_value,
    w_igate,
    w_fgate,
    forget_bias,
    gate_drift,
    head_gain,
    w_out,
):
    heads = w_igate.shape[1]
    if heads != 2 * tp or gate_drift.shape[0] > drift_span:
        return on_device(
            tokens,
            pre_gain,
            w_query,
            w_key,
            w_value,
            w_igate,
            w_fgate,
            forget_bias,
            gate_drift,
            head_gain,
            w_out,
        )
    rows, width = tokens.shape
    length = 2 * rows * tp
    q = n // 2
    steps = q - 1
    half_tp = tp // 2
    dk = w_query.shape[1] // 2
    dv = w_value.shape[1] // 2
    features = w_out.shape[0] * n
    vmem = pl.BlockSpec(memory_space=pltpu.VMEM)
    dma = pltpu.SemaphoreType.DMA
    weights = (w_key, w_value, w_query, w_out)
    smem = pl.BlockSpec(memory_space=pltpu.SMEM)
    return pl.pallas_call(
        functools.partial(square_kernel, n, tp),
        out_shape=jax.ShapeDtypeStruct((rows, features), bf16),
        in_specs=[vmem] * 7 + [smem] + [vmem] * 3,
        out_specs=vmem,
        scratch_shapes=[
            pltpu.VMEM((length, width), bf16),
            pltpu.VMEM((2, heads, gate_drift.shape[0]), f32),
            pltpu.VMEM((length, width), bf16),
            *[pltpu.VMEM((2, w.shape[0], w.shape[1] // 2), bf16) for w in weights],
            *[
                pltpu.VMEM((2, 2, steps, w.shape[0] // 2, w.shape[1] // 2), bf16)
                for w in weights
            ],
            pltpu.VMEM((dk, dv), bf16),
            pltpu.VMEM((steps, dk, dv), bf16),
            pltpu.VMEM((8, dk), f32),
            pltpu.VMEM((steps, 8, dk), f32),
            pltpu.VMEM((length, 2 * dk + dv), f32),
            pltpu.VMEM((length, dv), bf16),
            pltpu.VMEM((2, length, features // 2), bf16),
            pltpu.VMEM((2, length // 2, features // 2), bf16),
            pltpu.VMEM((2, length // 2, features // 2), bf16),
            pltpu.VMEM((2, half_tp - 1, 2 * rows, features // 2), bf16),
            pltpu.VMEM((2, 2 * rows, features // 2), bf16),
            pltpu.VMEM((2, 2, rows, features // 2), bf16),
            dma((2,)),
            dma((2,)),
            dma((2,)),
            dma((2,)),
            dma((2, half_tp)),
            dma((2, half_tp)),
            dma((2, half_tp)),
            dma((2, half_tp)),
            dma((2, 4)),
            dma((2, 4)),
            dma((4, 2, 2, steps)),
            dma((4, 2, 2, steps)),
            dma((steps,)),
            dma((steps,)),
            dma((steps,)),
            dma((steps,)),
            dma((2,)),
            dma((2,)),
            dma((2, half_tp)),
            dma((2, half_tp)),
            dma((2, 2)),
            dma((2, 2)),
        ],
        compiler_params=pltpu.CompilerParams(collective_id=0, has_side_effects=True),
    )(
        tokens,
        pre_gain,
        w_query,
        w_key,
        w_value,
        w_igate.T,
        w_fgate.T,
        forget_bias,
        gate_drift.T,
        head_gain,
        w_out,
    )


def solution(mesh):
    in_specs = (
        P(("sp", "tp"), None),
        P(),
        P("sp", "tp"),
        P("sp", "tp"),
        P("sp", "tp"),
        P(),
        P(),
        P(),
        P("sp", None),
        P(),
        P("sp", "tp"),
    )
    out_specs = P(("sp", "tp"), None)
    body = on_device
    if mesh.shape["sp"] <= ring_limit and mesh.shape["sp"] % 4 == 0 and mesh.shape["tp"] % 4 == 0:
        body = functools.partial(on_device_ring, mesh.shape["sp"], mesh.shape["tp"])
    return jax.shard_map(
        body, mesh=mesh, in_specs=in_specs, out_specs=out_specs, check_vma=False
    )
```
